32 devices in a mesh: grp: 2 (over y), fs: 4 (over z), tp: 4 (over x, core).
Axes of the slice: x: 2, y: 2, z: 4, core: 2. Of those that a mesh axis runs over, the one named last changes fastest.
Arguments:
- tokens: bfloat16 [4096, 2048], P(('grp', 'tp')), parts along dimension 0, may hold values from -6 to 6
- gate_weight: float32 [2, 2048, 5632], P(None, 'fs', 'tp'), may hold values from -0.125 to 0.125
- up_weight: float32 [2, 2048, 5632], P(None, 'fs', 'tp'), may hold values from -0.125 to 0.125
- down_weight: float32 [2, 2048, 5632], P(None, 'fs', 'tp'), may hold values from -0.078125 to 0.078125
- in_gain: float32 [2, 2048], P(None, 'fs'), may hold values from 0.1 to 1.9
- out_gain: float32 [2, 2048], replicated, may hold values from 0.1 to 1.9
Outputs:
- sampler_gate: bfloat16 [4, 2048, 5632], P('grp', None, 'fs'), parts along dimension 0
- sampler_up: bfloat16 [4, 2048, 5632], P('grp', None, 'fs'), parts along dimension 0
- sampler_down: bfloat16 [4, 2048, 5632], P('grp', None, 'fs'), parts along dimension 0
- result: bfloat16 [4096, 2048], P(('grp', 'tp', 'fs')), parts along dimension 0
The draws below stay inside these ranges and needn't reach their ends.
There are 2 independent parts, one for each index of `grp`. The reference program is written for one: setup_inputs(seed, part) draws one part's arguments, and reference() takes and returns one part's arrays. A program takes and returns all parts, laid end to end along the dimension named above; an argument that names none is the same for every part. Nothing has to cross between parts.
All inputs are finite; a program needn't handle non-finite values.
Results may differ from the reference program's by a relative error of at most 0.0073.
Values may be sent and summed in bfloat16 or wider, within the bound.
A program may use at most 192 MiB of HBM per device.

```python
import jax
import jax.numpy as jnp
from jax import lax

D = 2048
FF = 5632
TOKENS = 2048
HB = 352
N_FS = 4
N_TP = 4


def levels(stream_key, extent, shards, least, largest):
    loudness, own = 1.0, jax.random.fold_in(stream_key, 6)
    for position, shards_of in shards:
        draws = jnp.exp(jax.random.uniform(jax.random.fold_in(own, position), (shards_of,), jnp.float32, least / len(shards), largest / len(shards)))
        loudness = loudness * jnp.repeat(draws, extent[position] // shards_of).reshape([-1 if axis == position else 1 for axis in range(len(extent))])
    return loudness


def centred(stream_key, dims, width, bound, pieces=(), kind=jnp.bfloat16):
    entries = width * jax.random.normal(stream_key, dims, jnp.float32)
    if pieces:
        entries = entries * levels(stream_key, dims, pieces, -0.22, 0.18)
    return jnp.clip(entries, -bound, bound).astype(kind)


def setup_inputs(seed: int = 0, part: int = 0) -> dict:
    arg_keys = jax.random.split(jax.random.key(seed), 7)
    own_keys = jax.random.split(jax.random.fold_in(arg_keys[6], part), 7)
    return {
        "tokens": centred(own_keys[0], (TOKENS, D), 1.0, 6.0, ((0, 4),)),
        "gate_weight": centred(arg_keys[1], (2, D, FF), D ** -0.5, 0.125, ((1, 4), (2, 4)), jnp.float32),
        "up_weight": centred(arg_keys[2], (2, D, FF), D ** -0.5, 0.125, ((1, 4), (2, 4)), jnp.float32),
        "down_weight": centred(arg_keys[3], (2, D, FF), FF ** -0.5, 0.078125, ((1, 4), (2, 4)), jnp.float32),
        "in_gain": jnp.clip(1.0 + 0.18 * jax.random.normal(arg_keys[4], (2, D), jnp.float32), 0.1, 1.9),
        "out_gain": jnp.clip(1.0 + 0.18 * jax.random.normal(arg_keys[5], (2, D), jnp.float32), 0.1, 1.9),
    }


EPS = 1e-06

def normalize(rows):
    return rows * lax.rsqrt(lax.optimization_barrier(jnp.mean(rows * rows, axis=-1, keepdims=True)) + EPS)

def reorder(matrix):
    return matrix.reshape(D, N_TP, N_FS, HB).transpose(0, 2, 1, 3).reshape(D, FF)

def reference(tokens, gate_weight, up_weight, down_weight, in_gain, out_gain):
    gates = []
    ups = []
    downs = []
    state = tokens.astype(jnp.float32)
    rounded = tokens
    for section_idx in range(2):
        gate_matrix = (in_gain[section_idx][:, None] * gate_weight[section_idx]).astype(jnp.bfloat16)
        up_matrix = (in_gain[section_idx][:, None] * up_weight[section_idx]).astype(jnp.bfloat16)
        down_matrix = down_weight[section_idx].astype(jnp.bfloat16)
        gates.append(reorder(gate_matrix))
        ups.append(reorder(up_matrix))
        downs.append(reorder(down_matrix))
        normed = normalize(state).astype(jnp.bfloat16)
        gate_act = jnp.dot(normed, gate_matrix, preferred_element_type=jnp.float32)
        up_act = jnp.dot(normed, up_matrix, preferred_element_type=jnp.float32)
        hidden = (jax.nn.silu(gate_act) * up_act).astype(jnp.bfloat16)
        mixed = lax.dot_general(hidden, down_matrix, (((1,), (1,)), ((), ())), preferred_element_type=jnp.float32)
        rounded = lax.optimization_barrier((state + 0.5 * out_gain[section_idx] * normalize(mixed)).astype(jnp.bfloat16))
        state = rounded.astype(jnp.float32)
    return (jnp.stack(gates), jnp.stack(ups), jnp.stack(downs), rounded)
```

```python
import functools

import jax
import jax.numpy as jnp
from jax import lax
from jax.experimental import pallas as pl
from jax.experimental.pallas import tpu as pltpu
from jax.sharding import PartitionSpec as P

EPS = 1e-06


def normalize(rows):
    return rows * lax.rsqrt(jnp.mean(rows * rows, axis=-1, keepdims=True) + EPS)


def body_plain(tokens, gate_weight, up_weight, down_weight, in_gain, out_gain):
    groups = lax.axis_size("fs")
    rows_all = tokens.shape[0]
    rows_mine = rows_all // groups
    model_width = tokens.shape[1]
    local_rows = gate_weight.shape[1]
    block_width = gate_weight.shape[2] // groups
    residual = lax.dynamic_slice_in_dim(
        tokens, lax.axis_index("fs") * rows_mine, rows_mine, 0
    ).astype(jnp.float32)
    normed = normalize(tokens.astype(jnp.float32)).astype(jnp.bfloat16)
    gates = []
    ups = []
    downs = []
    rounded_state = tokens
    contract_last = (((1,), (1,)), ((), ()))
    for section_idx in range(2):
        scale = in_gain[section_idx][:, None]
        gate_rounded = (scale * gate_weight[section_idx]).astype(jnp.bfloat16)
        up_rounded = (scale * up_weight[section_idx]).astype(jnp.bfloat16)
        down_rounded = down_weight[section_idx].astype(jnp.bfloat16)
        flipped = [
            w.T.reshape(groups, block_width, local_rows)
            for w in (gate_rounded, up_rounded, down_rounded)
        ]
        arrived = (
            lax.all_to_all(flipped[0], "fs", split_axis=0, concat_axis=2, tiled=True),
            lax.all_to_all(flipped[1], "fs", split_axis=0, concat_axis=2, tiled=True),
            lax.all_to_all(flipped[2], "fs", split_axis=0, concat_axis=2, tiled=True),
        )
        thin_rows = [w.reshape(block_width, model_width) for w in arrived]
        sampler_mats = (
            lax.all_gather(thin_rows[0], "tp", axis=0, tiled=True),
            lax.all_gather(thin_rows[1], "tp", axis=0, tiled=True),
            lax.all_gather(thin_rows[2], "tp", axis=0, tiled=True),
        )
        gate_flip, up_flip, down_flip = (sampler_mats[0], sampler_mats[1], sampler_mats[2])
        gates.append(gate_flip.T)
        ups.append(up_flip.T)
        downs.append(down_flip.T)

        def hidden_of(row_block):
            gate_act = lax.dot_general(
                row_block, gate_flip, contract_last, preferred_element_type=jnp.float32
            )
            up_act = lax.dot_general(
                row_block, up_flip, contract_last, preferred_element_type=jnp.float32
            )
            return (jax.nn.silu(gate_act) * up_act).astype(jnp.bfloat16)

        if section_idx == 0:
            hidden = hidden_of(normed)
        else:
            hidden = hidden_of(lax.all_gather(normed, "fs", axis=0, tiled=True))
        mixed = lax.psum_scatter(
            jnp.dot(hidden, down_flip, preferred_element_type=jnp.float32),
            "fs",
            scatter_dimension=0,
            tiled=True,
        )
        rounded_state = (residual + 0.5 * out_gain[section_idx] * normalize(mixed)).astype(
            jnp.bfloat16
        )
        if section_idx == 0:
            residual = rounded_state.astype(jnp.float32)
            normed = normalize(residual).astype(jnp.bfloat16)
    return (jnp.stack(gates), jnp.stack(ups), jnp.stack(downs), rounded_state)


ORDER = (0, 3, 1, 2)
TURNED = ((0, 3), (2, 3), (4, 3))
LAST = (((1,), (1,)), ((), ()))
MESH = pl.DeviceIdType.MESH


def cuts(extent, width):
    return [(start, min(width, extent - start)) for start in range(0, extent, width)]


def fused_kernel(tokens, gate_w, up_w, down_w, in_gain, out_gain, *refs):
    full, state = refs[:6], refs[6]
    stage, flip, tok, normed, hidden, part, rin, lin, rout, lout, rs_r, rs_l = refs[7:19]
    load_sem, tok_sem, send_sem, recv_sem = refs[19:]
    y, z, t = lax.axis_index("grp"), lax.axis_index("fs"), lax.axis_index("tp")
    x, c = t // 2, lax.rem(t, 2)
    other_y, other_x, other_c = 1 - y, (1 - x) * 2 + c, x * 2 + (1 - c)
    other_both = (1 - x) * 2 + (1 - c)
    groups = 4
    ahead, behind = lax.rem(z + 1, groups), lax.rem(z + groups - 1, groups)
    to_x, to_c, to_y = {"tp": other_x}, {"tp": other_c}, {"grp": other_y}
    to_right, to_left = {"fs": ahead}, {"fs": behind}
    inner = (z > 0) & (z < groups - 1)
    _, rows, cols = gate_w.shape
    half_rows = rows // 2
    block = cols // groups
    half = block // 2
    count, width = tokens.shape
    quarter = count // groups
    piece = count // 8
    f32, bf16 = jnp.float32, jnp.bfloat16
    weights = (gate_w, up_w, down_w)

    names = []
    sent = []

    def slot(name):
        if name not in names:
            names.append(name)
        return names.index(name)

    def remote(name, source, target, device):
        k = slot(name)
        return pltpu.make_async_remote_copy(
            src_ref=source,
            dst_ref=target,
            send_sem=send_sem.at[k],
            recv_sem=recv_sem.at[k],
            device_id=device,
            device_id_type=MESH,
        )

    def send(name, source, target, device):
        copy = remote(name, source, target, device)
        copy.start()
        return copy

    def arrived(name, landed, device):
        remote(name, landed, landed, device).wait_recv()

    def slabs(start, extent, step, work):
        def one(i, carry):
            work(pl.ds(pl.multiple_of(start + i * step, step), step))
            return carry

        lax.fori_loop(0, extent // step, one, 0)

    def place(m, column, which, source):
        top = pl.multiple_of(column * block + which * half, 16)
        return full[m].at[pl.ds(top, half), pl.ds(pl.multiple_of(source * rows, 128), rows)]

    def blocks_of(m, column, source):
        top = pl.multiple_of(column * block, 16)
        return full[m].at[pl.ds(top, block), pl.ds(pl.multiple_of(source * rows, 128), rows)]

    def rows_of(m, column):
        return full[m].at[pl.ds(pl.multiple_of(column * block, 16), block), :]

    def origin(shift):
        return lax.rem(z + groups - shift, groups)

    def load(k):
        m, r = k // 2, k % 2
        return pltpu.make_async_copy(
            weights[m % 3].at[m // 3, pl.ds(r * half_rows, half_rows), :],
            stage.at[k % 2],
            load_sem.at[k % 2],
        )

    fetch = []
    for p, chunk in enumerate(ORDER):
        fetch.append(
            pltpu.make_async_copy(
                tokens.at[pl.ds(chunk * quarter, quarter), :],
                tok.at[pl.ds(p * quarter, quarter), :],
                tok_sem.at[p],
            )
        )
    load(0).start()
    load(1).start()
    for copy in fetch:
        copy.start()

    partners = [{"fs": lax.rem(z + shift, groups)} for shift in range(1, groups)]
    partners += [to_x, to_c, to_y]
    barrier = pltpu.get_barrier_semaphore()
    for partner in partners:
        pl.semaphore_signal(barrier, inc=1, device_id=partner, device_id_type=MESH)

    z_sends = {}

    def prep(m):
        layer, which, s = m // 3, m % 3, m % 3
        if m >= 3:
            for copy in z_sends[m - 3]:
                copy.wait_send()
        for r in range(2):
            k = 2 * m + r
            load(k).wait()
            lanes = slice(r * half_rows, (r + 1) * half_rows)

            def one(i, carry):
                cut = pl.ds(pl.multiple_of(i * 128, 128), 128)
                turned = stage[k % 2, :, cut].T
                if which < 2:
                    turned = turned * in_gain[layer : layer + 1, lanes]
                flip[s, cut, lanes] = turned.astype(bf16)
                return carry

            lax.fori_loop(0, cols // 128, one, 0)
            if k + 2 < 12:
                load(k + 2).start()
        mine = flip[s, pl.ds(pl.multiple_of(z * block, 16), block), :]
        top = pl.multiple_of(t * block, 16)
        full[m][pl.ds(top, block), pl.ds(pl.multiple_of(z * rows, 128), rows)] = mine

    def send_z(m):
        z_sends[m] = []
        for shift in range(1, groups):
            target = lax.rem(z + shift, groups)
            top = pl.multiple_of(target * block + y * half, 16)
            source = flip.at[m % 3, pl.ds(top, half), :]
            z_sends[m].append(send(("z", m, shift), source, place(m, t, y, z), {"fs": target}))

    def send_x(m):
        spot = blocks_of(m, t, z)
        sent.append(send(("x", m, 0), spot, spot, to_x))

    def on_z(m, shift):
        source = origin(shift)
        spot = place(m, t, y, source)
        arrived(("z", m, shift), spot, {"fs": source})
        sent.append(send(("x", m, shift), spot, spot, to_x))
        sent.append(send(("y", m, shift), spot, spot, to_y))

    def on_x(m, shift):
        source = origin(shift)
        spot = place(m, other_x, y, source)
        arrived(("x", m, shift), spot, to_x)
        if (m, shift) not in TURNED:
            sent.append(send(("w", m, shift), spot, spot, to_y))

    def finish(m):
        arrived(("x", m, 0), blocks_of(m, other_x, z), to_x)
        for shift in range(1, groups):
            spot = place(m, t, other_y, origin(shift))
            arrived(("y", m, shift), spot, to_y)
            if (m, shift) in TURNED:
                sent.append(send(("w", m, shift), spot, spot, to_x))
        mine = rows_of(m, t)
        sent.append(send(("c", m, 0), mine, mine, to_c))
        for shift in range(1, groups):
            device = to_x if (m, shift) in TURNED else to_y
            arrived(("w", m, shift), place(m, other_x, other_y, origin(shift)), device)
        mine = rows_of(m, other_x)
        sent.append(send(("c", m, 1), mine, mine, to_c))

    def on_c(m):
        arrived(("c", m, 0), rows_of(m, other_c), to_c)
        arrived(("c", m, 1), rows_of(m, other_both), to_c)

    def scaled(value):
        return value * lax.rsqrt(jnp.mean(value * value, axis=-1, keepdims=True) + EPS)

    def gated(layer, start, extent, cut):
        first, size = cut
        line = normed[start : start + extent, :]
        gate = lax.dot_general(
            line, full[3 * layer][first : first + size, :], LAST, preferred_element_type=f32
        )
        lift = lax.dot_general(
            line, full[3 * layer + 1][first : first + size, :], LAST, preferred_element_type=f32
        )
        value = jax.nn.silu(gate) * lift
        hidden[start : start + extent, first : first + size] = value.astype(bf16)

    def summed(layer, start, extent):
        line = hidden[start : start + extent, :]
        for first, size in cuts(width, 512):
            part[start : start + extent, first : first + size] = jnp.dot(
                line, full[3 * layer + 2][:, first : first + size], preferred_element_type=f32
            ).astype(bf16)

    def add_into(target, landed, offset, start, extent):
        def work(line):
            other = landed[line, :] if offset is None else landed[offset, line, :]
            total = other.astype(f32) + part[line, :].astype(f32)
            target[line, :] = total.astype(bf16)

        slabs(start, extent, 32, work)

    def lines(j):
        return pl.ds(j * piece, piece)

    def pass_right(j):
        arrived(("R", j), rin.at[lines(j), :], to_left)
        add_into(rout, rin, None, j * piece, piece)
        send(("R", j), rout.at[lines(j), :], rin.at[lines(j), :], to_right)

    def pass_left(j):
        arrived(("L", j), lin.at[lines(j), :], to_right)
        add_into(lout, lin, None, j * piece, piece)
        send(("L", j), lout.at[lines(j), :], lin.at[lines(j), :], to_left)

    def near(j):
        @pl.when(z == 1)
        def _():
            pass_right(j)

        @pl.when(z == 2)
        def _():
            pass_left(j)

    def edge(j):
        @pl.when(z == 0)
        def _():
            send(("R", j), part.at[lines(j), :], rin.at[lines(j), :], to_right)

        @pl.when(z == groups - 1)
        def _():
            send(("L", j), part.at[lines(j), :], lin.at[lines(j), :], to_left)

    def far(j):
        @pl.when(z == 1)
        def _():
            pass_left(j)

        @pl.when(z == 2)
        def _():
            pass_right(j)

    def settle(j):
        @pl.when(z == 0)
        def _():
            arrived(("L", j), lin.at[lines(j), :], to_right)

        @pl.when(z == groups - 1)
        def _():
            arrived(("R", j), rin.at[lines(j), :], to_left)

        def work(line):
            total = part[line, :].astype(f32) + rin[line, :].astype(f32) + lin[line, :].astype(f32)
            after = tok[line, :].astype(f32) + 0.5 * out_gain[0:1, :] * scaled(total)
            after = after.astype(bf16)
            tok[line, :] = after
            normed[line, :] = scaled(after.astype(f32)).astype(bf16)

        slabs(j * piece, piece, 32, work)

    def exchange(i):
        if i < 8:
            near(i)
        if 0 <= i - 1 < 8:
            far(i - 1)
        if 0 <= i - 2 < 8:
            settle(i - 2)

    def exchange_sent():
        for j in range(8):

            @pl.when(z < groups - 1)
            def _():
                remote(("R", j), rout.at[lines(j), :], rin.at[lines(j), :], to_right).wait_send()

            @pl.when(z > 0)
            def _():
                remote(("L", j), lout.at[lines(j), :], lin.at[lines(j), :], to_left).wait_send()

    def block_at(k):
        return pl.ds(ORDER.index(k) * quarter, quarter)

    def reduce_right(k):
        start = ORDER.index(k) * quarter

        @pl.when(z == 0)
        def _():
            send(("r", k), part.at[block_at(k), :], rs_r.at[block_at(k), :], to_right)

        @pl.when((z > 0) & (z < k))
        def _():
            arrived(("r", k), rs_r.at[block_at(k), :], to_left)
            add_into(rout, rs_r, None, start, quarter)
            send(("r", k), rout.at[block_at(k), :], rs_r.at[block_at(k), :], to_right)

    def reduce_left(k):
        start = ORDER.index(k) * quarter

        @pl.when(z == groups - 1)
        def _():
            send(("l", k), part.at[block_at(k), :], rs_l.at[block_at(k), :], to_left)

        @pl.when((z < groups - 1) & (z > k))
        def _():
            arrived(("l", k), rs_l.at[block_at(k), :], to_right)
            add_into(lout, rs_l, None, start, quarter)
            send(("l", k), lout.at[block_at(k), :], rs_l.at[block_at(k), :], to_left)

    def conclude():
        for k in range(groups):

            @pl.when(z == k)
            def _():
                if k > 0:
                    arrived(("r", k), rs_r.at[block_at(k), :], to_left)
                if k < groups - 1:
                    arrived(("l", k), rs_l.at[block_at(k), :], to_right)
                start = ORDER.index(k) * quarter

                def work(line):
                    total = part[line, :].astype(f32)
                    if k > 0:
                        total += rs_r[line, :].astype(f32)
                    if k < groups - 1:
                        total += rs_l[line, :].astype(f32)
                    after = tok[line, :].astype(f32) + 0.5 * out_gain[1:2, :] * scaled(total)
                    state[pl.ds(line.start - start, 32), :] = after.astype(bf16)

                slabs(start, quarter, 32, work)

        for k in range(1, groups):

            @pl.when(z < k)
            def _():
                remote(("r", k), rout.at[block_at(k), :], rout.at[block_at(k), :], to_right).wait_send()

        for k in range(groups - 1):

            @pl.when(z > k)
            def _():
                remote(("l", k), lout.at[block_at(k), :], lout.at[block_at(k), :], to_left).wait_send()

    prep(0)
    pl.semaphore_wait(barrier, len(partners))
    send_z(0)
    send_x(0)
    for m in (1, 2):
        prep(m)
        send_z(m)
        send_x(m)
    for copy in fetch:
        copy.wait()

    def first_norm(line):
        normed[line, :] = scaled(tok[line, :].astype(f32)).astype(bf16)

    slabs(0, count, 32, first_norm)

    @pl.when(z == 0)
    def _():
        rin[...] = jnp.zeros_like(rin)

    @pl.when(z == groups - 1)
    def _():
        lin[...] = jnp.zeros_like(lin)

    pieces = cuts(cols, 384)
    whole = (0, count)
    upper, lower = (0, count // 2), (count // 2, count // 2)

    on_z(0, 1)
    on_z(0, 2)
    on_x(0, 1)
    on_z(0, 3)
    on_x(0, 2)
    on_z(1, 1)
    on_x(0, 3)
    prep(3)
    send_z(3)
    send_x(3)
    on_z(1, 2)
    on_x(1, 1)
    on_z(1, 3)
    on_x(1, 2)
    finish(0)
    on_z(2, 1)
    on_x(1, 3)
    on_z(2, 2)
    on_x(2, 1)
    on_z(2, 3)
    prep(4)
    send_z(4)
    send_x(4)
    finish(1)
    on_x(2, 2)
    on_z(3, 1)
    on_c(0)
    on_c(1)
    gated(0, *whole, pieces[0])
    on_x(2, 3)
    on_z(3, 2)
    gated(0, *whole, pieces[1])
    on_z(3, 3)
    on_x(3, 1)
    gated(0, *whole, pieces[2])
    gated(0, *whole, pieces[3])
    finish(2)
    on_x(3, 2)
    on_c(2)
    summed(0, *upper)
    for j in range(4):
        edge(j)
    summed(0, *lower)
    for j in range(4, 8):
        edge(j)
    on_z(4, 1)
    on_x(3, 3)
    on_z(4, 2)
    on_x(4, 1)
    on_z(4, 3)
    prep(5)
    exchange(0)
    finish(3)
    exchange(1)
    on_x(4, 2)
    exchange(2)
    send_z(5)
    send_x(5)
    on_x(4, 3)
    exchange(3)
    exchange(4)
    on_z(5, 1)
    exchange(5)
    on_z(5, 2)
    on_x(5, 1)
    finish(4)
    exchange(6)
    on_z(5, 3)
    on_x(5, 2)
    on_c(3)
    on_c(4)
    exchange(7)
    for cut in pieces:
        gated(1, *upper, cut)
    on_x(5, 3)
    exchange(8)
    exchange(9)
    for cut in pieces:
        gated(1, *lower, cut)
    exchange_sent()
    finish(5)
    on_c(5)
    summed(1, *upper)
    reduce_right(3)
    reduce_left(0)
    summed(1, *lower)
    reduce_right(2)
    reduce_left(1)
    reduce_right(1)
    reduce_left(2)
    conclude()
    for m in (3, 4, 5):
        sent.extend(z_sends[m])
    for copy in sent:
        copy.wait_send()


def fused(tokens, gate_weight, up_weight, down_weight, in_gain, out_gain):
    count, width = tokens.shape
    _, rows, cols = gate_weight.shape
    bf16 = jnp.bfloat16
    quarter = count // 4
    whole = pl.BlockSpec(memory_space=pl.ANY)
    near = pl.BlockSpec(memory_space=pltpu.VMEM)
    band = pltpu.VMEM((count, width), bf16)
    messages = 128
    return pl.pallas_call(
        fused_kernel,
        in_specs=[whole] * 4 + [near] * 2,
        out_specs=[near] * 7,
        out_shape=[pltpu.VMEM((cols, width), bf16)] * 6 + [pltpu.VMEM((quarter, width), bf16)],
        scratch_shapes=[
            pltpu.VMEM((2, rows // 2, cols), jnp.float32),
            pltpu.VMEM((3, cols, rows), bf16),
            band,
            band,
            pltpu.VMEM((count, cols), bf16),
            band,
            band,
            band,
            band,
            band,
            band,
            band,
            pltpu.SemaphoreType.DMA((2,)),
            pltpu.SemaphoreType.DMA((4,)),
            pltpu.SemaphoreType.DMA((messages,)),
            pltpu.SemaphoreType.DMA((messages,)),
        ],
        compiler_params=pltpu.CompilerParams(
            collective_id=0, has_side_effects=True, vmem_limit_bytes=29 * 2**20
        ),
    )(tokens, gate_weight, up_weight, down_weight, in_gain, out_gain)


def emit_kernel(*refs):
    flips, state = refs[:6], refs[6]
    outs, result = refs[7:10], refs[10]
    held, sems, state_sem = refs[11:]
    slots, step, _ = held.shape
    width = flips[0].shape[1]
    steps = width // step
    last = pltpu.make_async_copy(state, result, state_sem)
    last.start()

    def out_copy(k, i):
        slot = lax.rem(i, slots)
        top = pl.multiple_of(i * step, step)
        return pltpu.make_async_copy(
            held.at[slot], outs[k % 3].at[k // 3, pl.ds(top, step), :], sems.at[slot]
        )

    for k in range(6):

        def one(i, carry):
            if k == 0:

                @pl.when(i >= slots)
                def _():
                    out_copy(k, i).wait()

            else:
                out_copy(k, i).wait()
            held[lax.rem(i, slots)] = flips[k][:, pl.ds(pl.multiple_of(i * step, step), step)].T
            out_copy(k, i).start()
            return carry

        lax.fori_loop(0, steps, one, 0)
    for i in range(slots):
        out_copy(5, steps - slots + i).wait()
    last.wait()


def emit(flips, state):
    cols, width = flips[0].shape
    near = pl.BlockSpec(memory_space=pltpu.VMEM)
    whole = pl.BlockSpec(memory_space=pl.ANY)
    return pl.pallas_call(
        emit_kernel,
        in_specs=[near] * 7,
        out_specs=[whole] * 4,
        out_shape=[jax.ShapeDtypeStruct((2, width, cols), jnp.bfloat16)] * 3
        + [jax.ShapeDtypeStruct(state.shape, jnp.bfloat16)],
        scratch_shapes=[
            pltpu.VMEM((8, 256, cols), jnp.bfloat16),
            pltpu.SemaphoreType.DMA((8,)),
            pltpu.SemaphoreType.DMA,
        ],
        compiler_params=pltpu.CompilerParams(vmem_limit_bytes=16 * 2**20),
    )(*flips, state)


def body(tokens, gate_weight, up_weight, down_weight, in_gain, out_gain):
    groups, halves = lax.axis_size("fs"), lax.axis_size("grp")
    columns = lax.axis_size("tp")
    count, model_width = tokens.shape
    _, rows, cols = gate_weight.shape
    odd = cols % (32 * groups) or rows % 256 or cols % 128 or count % 512 or model_width % 2048
    if odd or halves != 2 or columns != 4 or groups != 4:
        return body_plain(tokens, gate_weight, up_weight, down_weight, in_gain, out_gain)
    *flips, state = fused(tokens, gate_weight, up_weight, down_weight, in_gain, out_gain)
    return tuple(emit(flips, state))


def solution(mesh):
    in_specs = (
        P(("grp", "tp"), None),
        P(None, "fs", "tp"),
        P(None, "fs", "tp"),
        P(None, "fs", "tp"),
        P(None, "fs"),
        P(),
    )
    out_specs = (
        P("grp", None, "fs"),
        P("grp", None, "fs"),
        P("grp", None, "fs"),
        P(("grp", "tp", "fs"), None),
    )
    return jax.shard_map(body, mesh=mesh, in_specs=in_specs, out_specs=out_specs, check_vma=False)
```

```python
import functools

import jax
import jax.numpy as jnp
from jax import lax
from jax.experimental import pallas as pl
from jax.experimental.pallas import tpu as pltpu
from jax.sharding import PartitionSpec as P

EPS = 1e-06


def normalize(rows):
    return rows * lax.rsqrt(jnp.mean(rows * rows, axis=-1, keepdims=True) + EPS)


def body_plain(tokens, gate_weight, up_weight, down_weight, in_gain, out_gain):
    groups = lax.axis_size("fs")
    rows_all = tokens.shape[0]
    rows_mine = rows_all // groups
    model_width = tokens.shape[1]
    local_rows = gate_weight.shape[1]
    block_width = gate_weight.shape[2] // groups
    residual = lax.dynamic_slice_in_dim(
        tokens, lax.axis_index("fs") * rows_mine, rows_mine, 0
    ).astype(jnp.float32)
    normed = normalize(tokens.astype(jnp.float32)).astype(jnp.bfloat16)
    gates = []
    ups = []
    downs = []
    rounded_state = tokens
    contract_last = (((1,), (1,)), ((), ()))
    for section_idx in range(2):
        scale = in_gain[section_idx][:, None]
        gate_rounded = (scale * gate_weight[section_idx]).astype(jnp.bfloat16)
        up_rounded = (scale * up_weight[section_idx]).astype(jnp.bfloat16)
        down_rounded = down_weight[section_idx].astype(jnp.bfloat16)
        flipped = [
            w.T.reshape(groups, block_width, local_rows)
            for w in (gate_rounded, up_rounded, down_rounded)
        ]
        arrived = (
            lax.all_to_all(flipped[0], "fs", split_axis=0, concat_axis=2, tiled=True),
            lax.all_to_all(flipped[1], "fs", split_axis=0, concat_axis=2, tiled=True),
            lax.all_to_all(flipped[2], "fs", split_axis=0, concat_axis=2, tiled=True),
        )
        thin_rows = [w.reshape(block_width, model_width) for w in arrived]
        sampler_mats = (
            lax.all_gather(thin_rows[0], "tp", axis=0, tiled=True),
            lax.all_gather(thin_rows[1], "tp", axis=0, tiled=True),
            lax.all_gather(thin_rows[2], "tp", axis=0, tiled=True),
        )
        gate_flip, up_flip, down_flip = (sampler_mats[0], sampler_mats[1], sampler_mats[2])
        gates.append(gate_flip.T)
        ups.append(up_flip.T)
        downs.append(down_flip.T)

        def hidden_of(row_block):
            gate_act = lax.dot_general(
                row_block, gate_flip, contract_last, preferred_element_type=jnp.float32
            )
            up_act = lax.dot_general(
                row_block, up_flip, contract_last, preferred_element_type=jnp.float32
            )
            return (jax.nn.silu(gate_act) * up_act).astype(jnp.bfloat16)

        if section_idx == 0:
            hidden = hidden_of(normed)
        else:
            hidden = hidden_of(lax.all_gather(normed, "fs", axis=0, tiled=True))
        mixed = lax.psum_scatter(
            jnp.dot(hidden, down_flip, preferred_element_type=jnp.float32),
            "fs",
            scatter_dimension=0,
            tiled=True,
        )
        rounded_state = (residual + 0.5 * out_gain[section_idx] * normalize(mixed)).astype(
            jnp.bfloat16
        )
        if section_idx == 0:
            residual = rounded_state.astype(jnp.float32)
            normed = normalize(residual).astype(jnp.bfloat16)
    return (jnp.stack(gates), jnp.stack(ups), jnp.stack(downs), rounded_state)


ORDER = (0, 3, 1, 2)
TURNED = ((0, 1), (2, 1), (4, 1))
LAST = (((1,), (1,)), ((), ()))
MESH = pl.DeviceIdType.MESH


def cuts(extent, width):
    return [(start, min(width, extent - start)) for start in range(0, extent, width)]


def fused_kernel(tokens, gate_w, up_w, down_w, in_gain, out_gain, *refs):
    cols = gate_w.shape[2]
    full = [refs[0].at[pl.ds(m * cols, cols), :] for m in range(6)]
    state = refs[0]
    stage, flip, tok, normed, hidden, part, rin, lin, rout, lout, rs_r, rs_l = refs[1:13]
    load_sem, tok_sem, send_sem, recv_sem = refs[13:]
    y, z, t = lax.axis_index("grp"), lax.axis_index("fs"), lax.axis_index("tp")
    x, c = t // 2, lax.rem(t, 2)
    other_y, other_x, other_c = 1 - y, (1 - x) * 2 + c, x * 2 + (1 - c)
    other_both = (1 - x) * 2 + (1 - c)
    groups = 4
    ahead, behind = lax.rem(z + 1, groups), lax.rem(z + groups - 1, groups)
    to_x, to_c, to_y = {"tp": other_x}, {"tp": other_c}, {"grp": other_y}
    to_right, to_left = {"fs": ahead}, {"fs": behind}
    inner = (z > 0) & (z < groups - 1)
    _, rows, cols = gate_w.shape
    half_rows = rows // 2
    block = cols // groups
    half = block // 2
    count, width = tokens.shape
    quarter = count // groups
    piece = count // 8
    f32, bf16 = jnp.float32, jnp.bfloat16
    weights = (gate_w, up_w, down_w)

    names = []
    sent = []

    def slot(name):
        if name not in names:
            names.append(name)
        return names.index(name)

    def remote(name, source, target, device):
        k = slot(name)
        return pltpu.make_async_remote_copy(
            src_ref=source,
            dst_ref=target,
            send_sem=send_sem.at[k],
            recv_sem=recv_sem.at[k],
            device_id=device,
            device_id_type=MESH,
        )

    def send(name, source, target, device):
        copy = remote(name, source, target, device)
        copy.start()
        return copy

    def arrived(name, landed, device):
        remote(name, landed, landed, device).wait_recv()

    def slabs(start, extent, step, work):
        def one(i, carry):
            work(pl.ds(pl.multiple_of(start + i * step, step), step))
            return carry

        lax.fori_loop(0, extent // step, one, 0)

    def place(m, column, which, source):
        top = pl.multiple_of(column * block + which * half, 16)
        return full[m].at[pl.ds(top, half), pl.ds(pl.multiple_of(source * rows, 128), rows)]

    def blocks_of(m, column, source):
        top = pl.multiple_of(column * block, 16)
        return full[m].at[pl.ds(top, block), pl.ds(pl.multiple_of(source * rows, 128), rows)]

    def rows_of(m, column):
        return full[m].at[pl.ds(pl.multiple_of(column * block, 16), block), :]

    def origin(order):
        return (z + 1 - 2 * lax.rem(z, 2), 2 - z // 2, 3 * (1 - z // 2))[order - 1]

    def load(k):
        m, r = k // 2, k % 2
        return pltpu.make_async_copy(
            weights[m % 3].at[m // 3, pl.ds(r * half_rows, half_rows), :],
            stage.at[k % 2],
            load_sem.at[k % 2],
        )

    fetch = []
    for p, chunk in enumerate(ORDER):
        fetch.append(
            pltpu.make_async_copy(
                tokens.at[pl.ds(chunk * quarter, quarter), :],
                tok.at[pl.ds(p * quarter, quarter), :],
                tok_sem.at[p],
            )
        )
    load(0).start()
    load(1).start()
    for copy in fetch:
        copy.start()

    partners = [{"fs": lax.rem(z + shift, groups)} for shift in range(1, groups)]
    partners += [to_x, to_c, to_y]
    barrier = pltpu.get_barrier_semaphore()
    for partner in partners:
        pl.semaphore_signal(barrier, inc=1, device_id=partner, device_id_type=MESH)

    z_sends = {}

    def prep(m):
        layer, which, s = m // 3, m % 3, m % 3
        if m >= 3:
            for copy in z_sends[m - 3]:
                copy.wait_send()
        for r in range(2):
            k = 2 * m + r
            load(k).wait()
            lanes = slice(r * half_rows, (r + 1) * half_rows)

            def one(i, carry):
                cut = pl.ds(pl.multiple_of(i * 128, 128), 128)
                turned = stage[k % 2, :, cut].T
                if which < 2:
                    turned = turned * in_gain[layer : layer + 1, lanes]
                flip[s, cut, lanes] = turned.astype(bf16)
                return carry

            lax.fori_loop(0, cols // 128, one, 0)
            if k + 2 < 12:
                load(k + 2).start()
        mine = flip[s, pl.ds(pl.multiple_of(z * block, 16), block), :]
        top = pl.multiple_of(t * block, 16)
        full[m][pl.ds(top, block), pl.ds(pl.multiple_of(z * rows, 128), rows)] = mine

    def send_z(m):
        z_sends[m] = []
        base = [slot(("z", m, order)) for order in range(1, groups)][0]
        outer = 1 - (lax.rem(z, 3) + 1) // 2
        for order in range(1, groups):
            target = origin(order)
            top = pl.multiple_of(target * block + y * half, 16)
            landing = base if order == 1 else base + 1 + outer
            copy = pltpu.make_async_remote_copy(
                src_ref=flip.at[m % 3, pl.ds(top, half), :],
                dst_ref=place(m, t, y, z),
                send_sem=send_sem.at[base + order - 1],
                recv_sem=recv_sem.at[landing],
                device_id={"fs": target},
                device_id_type=MESH,
            )
            copy.start()
            z_sends[m].append(copy)

    def send_x(m):
        spot = blocks_of(m, t, z)
        sent.append(send(("x", m, 0), spot, spot, to_x))

    def on_z(m, shift):
        source = origin(shift)
        spot = place(m, t, y, source)
        arrived(("z", m, shift), spot, {"fs": source})
        sent.append(send(("x", m, shift), spot, spot, to_x))
        sent.append(send(("y", m, shift), spot, spot, to_y))

    def on_x(m, shift):
        spot = place(m, other_x, y, origin(shift))
        arrived(("x", m, shift), spot, to_x)
        sent.append(send(("w", m, shift), spot, spot, to_y))

    def turn(m, order):
        spot = place(m, t, other_y, origin(order))
        arrived(("y", m, order), spot, to_y)
        sent.append(send(("w", m, order), spot, spot, to_x))

    def finish(m):
        arrived(("x", m, 0), blocks_of(m, other_x, z), to_x)
        for shift in range(1, groups):
            if (m, shift) in TURNED:
                arrived(("x", m, shift), place(m, other_x, y, origin(shift)), to_x)
            else:
                arrived(("y", m, shift), place(m, t, other_y, origin(shift)), to_y)
        mine = rows_of(m, t)
        sent.append(send(("c", m, 0), mine, mine, to_c))
        for shift in range(1, groups):
            device = to_x if (m, shift) in TURNED else to_y
            arrived(("w", m, shift), place(m, other_x, other_y, origin(shift)), device)
        mine = rows_of(m, other_x)
        sent.append(send(("c", m, 1), mine, mine, to_c))

    def on_c(m):
        arrived(("c", m, 0), rows_of(m, other_c), to_c)
        arrived(("c", m, 1), rows_of(m, other_both), to_c)

    def scaled(value):
        return value * lax.rsqrt(jnp.mean(value * value, axis=-1, keepdims=True) + EPS)

    def gated(layer, start, extent, cut):
        first, size = cut
        line = normed[start : start + extent, :]
        gate = lax.dot_general(
            line, full[3 * layer][first : first + size, :], LAST, preferred_element_type=f32
        )
        lift = lax.dot_general(
            line, full[3 * layer + 1][first : first + size, :], LAST, preferred_element_type=f32
        )
        value = jax.nn.silu(gate) * lift
        hidden[start : start + extent, first : first + size] = value.astype(bf16)

    def summed(layer, start, extent):
        line = hidden[start : start + extent, :]
        for first, size in cuts(width, 512):
            part[start : start + extent, first : first + size] = jnp.dot(
                line, full[3 * layer + 2][:, first : first + size], preferred_element_type=f32
            ).astype(bf16)

    def add_into(target, landed, offset, start, extent):
        def work(line):
            other = landed[line, :] if offset is None else landed[offset, line, :]
            total = other.astype(f32) + part[line, :].astype(f32)
            target[line, :] = total.astype(bf16)

        slabs(start, extent, 32, work)

    def lines(j):
        return pl.ds(j * piece, piece)

    def pass_right(j):
        arrived(("R", j), rin.at[lines(j), :], to_left)
        add_into(rout, rin, None, j * piece, piece)
        send(("R", j), rout.at[lines(j), :], rin.at[lines(j), :], to_right)

    def pass_left(j):
        arrived(("L", j), lin.at[lines(j), :], to_right)
        add_into(lout, lin, None, j * piece, piece)
        send(("L", j), lout.at[lines(j), :], lin.at[lines(j), :], to_left)

    def near(j):
        @pl.when(z == 1)
        def _():
            pass_right(j)

        @pl.when(z == 2)
        def _():
            pass_left(j)

    def edge(j):
        @pl.when(z == 0)
        def _():
            send(("R", j), part.at[lines(j), :], rin.at[lines(j), :], to_right)

        @pl.when(z == groups - 1)
        def _():
            send(("L", j), part.at[lines(j), :], lin.at[lines(j), :], to_left)

    def far(j):
        @pl.when(z == 1)
        def _():
            pass_left(j)

        @pl.when(z == 2)
        def _():
            pass_right(j)

    def settle(j):
        @pl.when(z == 0)
        def _():
            arrived(("L", j), lin.at[lines(j), :], to_right)

        @pl.when(z == groups - 1)
        def _():
            arrived(("R", j), rin.at[lines(j), :], to_left)

        def work(line):
            total = part[line, :].astype(f32) + rin[line, :].astype(f32) + lin[line, :].astype(f32)
            after = tok[line, :].astype(f32) + 0.5 * out_gain[0:1, :] * scaled(total)
            after = after.astype(bf16)
            tok[line, :] = after
            normed[line, :] = scaled(after.astype(f32)).astype(bf16)

        slabs(j * piece, piece, 32, work)

    def exchange(i):
        if i < 8:
            near(i)
        if 0 <= i - 1 < 8:
            far(i - 1)
        if 0 <= i - 2 < 8:
            settle(i - 2)

    def exchange_sent(first, last):
        for j in range(first, last):

            @pl.when(z < groups - 1)
            def _():
                remote(("R", j), rout.at[lines(j), :], rin.at[lines(j), :], to_right).wait_send()

            @pl.when(z > 0)
            def _():
                remote(("L", j), lout.at[lines(j), :], lin.at[lines(j), :], to_left).wait_send()

    def parts_of(k):
        return [j for j in range(8) if ORDER[j // 2] == k]

    def reduce_edge(rightward, leftward):
        @pl.when(z == 0)
        def _():
            for j in parts_of(rightward):
                send(("r", j), part.at[lines(j), :], rs_r.at[lines(j), :], to_right)

        @pl.when(z == groups - 1)
        def _():
            for j in parts_of(leftward):
                send(("l", j), part.at[lines(j), :], rs_l.at[lines(j), :], to_left)

    def reduce_right(j):
        arrived(("r", j), rs_r.at[lines(j), :], to_left)
        add_into(rout, rs_r, None, j * piece, piece)
        send(("r", j), rout.at[lines(j), :], rs_r.at[lines(j), :], to_right)

    def reduce_left(j):
        arrived(("l", j), rs_l.at[lines(j), :], to_right)
        add_into(lout, rs_l, None, j * piece, piece)
        send(("l", j), lout.at[lines(j), :], rs_l.at[lines(j), :], to_left)

    def reduce_all():
        zeros, ones, twos, threes = [parts_of(k) for k in range(groups)]

        @pl.when(z == 1)
        def _():
            reduce_right(threes[0])
            reduce_right(threes[1])
            reduce_left(zeros[0])
            reduce_right(twos[0])
            reduce_left(zeros[1])
            reduce_right(twos[1])

        @pl.when(z == 2)
        def _():
            reduce_left(zeros[0])
            reduce_left(zeros[1])
            reduce_right(threes[0])
            reduce_left(ones[0])
            reduce_right(threes[1])
            reduce_left(ones[1])

    def conclude():
        for k in range(groups):
            for j in parts_of(k):

                @pl.when(z == k)
                def _():
                    if k > 0:
                        arrived(("r", j), rs_r.at[lines(j), :], to_left)
                    if k < groups - 1:
                        arrived(("l", j), rs_l.at[lines(j), :], to_right)
                    shift = 6 * cols - ORDER.index(k) * quarter

                    def work(line):
                        total = part[line, :].astype(f32)
                        if k > 0:
                            total += rs_r[line, :].astype(f32)
                        if k < groups - 1:
                            total += rs_l[line, :].astype(f32)
                        after = tok[line, :].astype(f32) + 0.5 * out_gain[1:2, :] * scaled(total)
                        state[pl.ds(line.start + shift, 32), :] = after.astype(bf16)

                    slabs(j * piece, piece, 32, work)

        for k in range(groups):
            for j in parts_of(k):

                @pl.when(z < k)
                def _():
                    remote(("r", j), rout.at[lines(j), :], rs_r.at[lines(j), :], to_right).wait_send()

                @pl.when(z > k)
                def _():
                    remote(("l", j), lout.at[lines(j), :], rs_l.at[lines(j), :], to_left).wait_send()

    prep(0)
    pl.semaphore_wait(barrier, len(partners))
    send_z(0)
    send_x(0)
    prep(1)
    prep(2)
    for copy in fetch:
        copy.wait()

    def first_norm(line):
        normed[line, :] = scaled(tok[line, :].astype(f32)).astype(bf16)

    on_z(0, 1)
    slabs(0, count, 32, first_norm)

    @pl.when(z == 0)
    def _():
        rin[...] = jnp.zeros_like(rin)

    @pl.when(z == groups - 1)
    def _():
        lin[...] = jnp.zeros_like(lin)

    pieces = cuts(cols, 384)
    whole = (0, count)
    upper, lower = (0, count // 2), (count // 2, count // 2)

    on_z(0, 2)
    send_z(1)
    turn(0, 1)
    on_z(0, 3)
    on_x(0, 2)
    on_x(0, 3)
    on_z(1, 1)
    on_z(1, 2)
    send_z(2)
    finish(0)
    on_x(1, 1)
    on_z(1, 3)
    send_x(1)
    on_x(1, 2)
    on_x(1, 3)
    on_z(2, 1)
    prep(3)
    on_z(2, 2)
    send_z(3)
    on_z(2, 3)
    prep(4)
    send_z(4)
    on_x(2, 2)
    finish(1)
    on_x(2, 3)
    turn(2, 1)
    send_x(2)
    on_z(3, 1)
    prep(5)
    on_c(0)
    on_c(1)
    gated(0, *whole, pieces[0])
    on_z(3, 2)
    send_z(5)
    gated(0, *whole, pieces[1])
    on_z(3, 3)
    gated(0, *whole, pieces[2])
    on_x(3, 1)
    gated(0, *whole, pieces[3])
    finish(2)
    on_x(3, 2)
    send_x(3)
    on_c(2)
    summed(0, *upper)
    for j in range(4):
        edge(j)
    summed(0, *lower)
    for j in range(4, 8):
        edge(j)
    on_x(3, 3)
    on_z(4, 1)
    on_z(4, 2)
    on_z(4, 3)
    exchange(0)
    finish(3)
    exchange(1)
    turn(4, 1)
    on_x(4, 2)
    exchange(2)
    on_x(4, 3)
    send_x(4)
    on_z(5, 1)
    on_z(5, 2)
    exchange(3)
    on_x(5, 1)
    on_z(5, 3)
    exchange(4)
    finish(4)
    send_x(5)
    exchange(5)
    on_x(5, 2)
    exchange(6)
    on_x(5, 3)
    on_c(3)
    on_c(4)
    for cut in pieces:
        gated(1, *upper, cut)
    exchange(7)
    finish(5)
    exchange(8)
    on_c(5)
    exchange_sent(0, 4)
    summed(1, *upper)
    reduce_edge(3, 0)
    exchange(9)
    for cut in pieces:
        gated(1, *lower, cut)
    exchange_sent(4, 8)
    summed(1, *lower)
    reduce_edge(2, 1)
    reduce_edge(1, 2)
    reduce_all()
    conclude()
    for m in (3, 4, 5):
        sent.extend(z_sends[m])
    for copy in sent:
        copy.wait_send()


def fused(tokens, gate_weight, up_weight, down_weight, in_gain, out_gain):
    count, width = tokens.shape
    _, rows, cols = gate_weight.shape
    bf16 = jnp.bfloat16
    quarter = count // 4
    whole = pl.BlockSpec(memory_space=pl.ANY)
    near = pl.BlockSpec(memory_space=pltpu.VMEM)
    band = pltpu.VMEM((count, width), bf16)
    messages = 128
    return pl.pallas_call(
        fused_kernel,
        in_specs=[whole] * 4 + [near] * 2,
        out_specs=near,
        out_shape=pltpu.VMEM((6 * cols + quarter, width), bf16),
        scratch_shapes=[
            pltpu.VMEM((2, rows // 2, cols), jnp.float32),
            pltpu.VMEM((3, cols, rows), bf16),
            band,
            band,
            pltpu.VMEM((count, cols), bf16),
            band,
            band,
            band,
            band,
            band,
            band,
            band,
            pltpu.SemaphoreType.DMA((2,)),
            pltpu.SemaphoreType.DMA((4,)),
            pltpu.SemaphoreType.DMA((messages,)),
            pltpu.SemaphoreType.DMA((messages,)),
        ],
        compiler_params=pltpu.CompilerParams(
            collective_id=0, has_side_effects=True, vmem_limit_bytes=29 * 2**20
        ),
    )(tokens, gate_weight, up_weight, down_weight, in_gain, out_gain)


def emit_kernel(flips, *refs):
    outs, result = refs[:3], refs[3]
    held, sems, state_sem = refs[4:]
    slots, step, cols = held.shape
    width = flips.shape[1]
    steps = width // step
    quarter = flips.shape[0] - 6 * cols
    last = pltpu.make_async_copy(flips.at[pl.ds(6 * cols, quarter), :], result, state_sem)
    last.start()

    def out_copy(k, i):
        slot = lax.rem(i, slots)
        top = pl.multiple_of(i * step, step)
        return pltpu.make_async_copy(
            held.at[slot], outs[k % 3].at[k // 3, pl.ds(top, step), :], sems.at[slot]
        )

    for k in range(6):

        def one(i, carry):
            if k == 0:

                @pl.when(i >= slots)
                def _():
                    out_copy(k, i).wait()

            else:
                out_copy(k, i).wait()
            lanes = pl.ds(pl.multiple_of(i * step, step), step)
            held[lax.rem(i, slots)] = flips[k * cols : (k + 1) * cols, lanes].T
            out_copy(k, i).start()
            return carry

        lax.fori_loop(0, steps, one, 0)
    for i in range(slots):
        out_copy(5, steps - slots + i).wait()
    last.wait()


def emit(flips, cols):
    height, width = flips.shape
    near = pl.BlockSpec(memory_space=pltpu.VMEM)
    whole = pl.BlockSpec(memory_space=pl.ANY)
    return pl.pallas_call(
        emit_kernel,
        in_specs=[near],
        out_specs=[whole] * 4,
        out_shape=[jax.ShapeDtypeStruct((2, width, cols), jnp.bfloat16)] * 3
        + [jax.ShapeDtypeStruct((height - 6 * cols, width), jnp.bfloat16)],
        scratch_shapes=[
            pltpu.VMEM((8, 256, cols), jnp.bfloat16),
            pltpu.SemaphoreType.DMA((8,)),
            pltpu.SemaphoreType.DMA,
        ],
        compiler_params=pltpu.CompilerParams(vmem_limit_bytes=8 * 2**20),
    )(flips)


def body(tokens, gate_weight, up_weight, down_weight, in_gain, out_gain):
    groups, halves = lax.axis_size("fs"), lax.axis_size("grp")
    columns = lax.axis_size("tp")
    count, model_width = tokens.shape
    _, rows, cols = gate_weight.shape
    odd = cols % (32 * groups) or rows % 256 or cols % 128 or count % 512 or model_width % 2048
    if odd or halves != 2 or columns != 4 or groups != 4:
        return body_plain(tokens, gate_weight, up_weight, down_weight, in_gain, out_gain)
    flips = fused(tokens, gate_weight, up_weight, down_weight, in_gain, out_gain)
    return tuple(emit(flips, cols))


def solution(mesh):
    in_specs = (
        P(("grp", "tp"), None),
        P(None, "fs", "tp"),
        P(None, "fs", "tp"),
        P(None, "fs", "tp"),
        P(None, "fs"),
        P(),
    )
    out_specs = (
        P("grp", None, "fs"),
        P("grp", None, "fs"),
        P("grp", None, "fs"),
        P(("grp", "tp", "fs"), None),
    )
    return jax.shard_map(body, mesh=mesh, in_specs=in_specs, out_specs=out_specs, check_vma=False)
```

```python
import functools

import jax
import jax.numpy as jnp
from jax import lax
from jax.experimental import pallas as pl
from jax.experimental.pallas import tpu as pltpu
from jax.sharding import PartitionSpec as P

EPS = 1e-06


def normalize(rows):
    return rows * lax.rsqrt(jnp.mean(rows * rows, axis=-1, keepdims=True) + EPS)


def body_plain(tokens, gate_weight, up_weight, down_weight, in_gain, out_gain):
    groups = lax.axis_size("fs")
    rows_all = tokens.shape[0]
    rows_mine = rows_all // groups
    model_width = tokens.shape[1]
    local_rows = gate_weight.shape[1]
    block_width = gate_weight.shape[2] // groups
    residual = lax.dynamic_slice_in_dim(
        tokens, lax.axis_index("fs") * rows_mine, rows_mine, 0
    ).astype(jnp.float32)
    normed = normalize(tokens.astype(jnp.float32)).astype(jnp.bfloat16)
    gates = []
    ups = []
    downs = []
    rounded_state = tokens
    contract_last = (((1,), (1,)), ((), ()))
    for section_idx in range(2):
        scale = in_gain[section_idx][:, None]
        gate_rounded = (scale * gate_weight[section_idx]).astype(jnp.bfloat16)
        up_rounded = (scale * up_weight[section_idx]).astype(jnp.bfloat16)
        down_rounded = down_weight[section_idx].astype(jnp.bfloat16)
        flipped = [
            w.T.reshape(groups, block_width, local_rows)
            for w in (gate_rounded, up_rounded, down_rounded)
        ]
        arrived = (
            lax.all_to_all(flipped[0], "fs", split_axis=0, concat_axis=2, tiled=True),
            lax.all_to_all(flipped[1], "fs", split_axis=0, concat_axis=2, tiled=True),
            lax.all_to_all(flipped[2], "fs", split_axis=0, concat_axis=2, tiled=True),
        )
        thin_rows = [w.reshape(block_width, model_width) for w in arrived]
        sampler_mats = (
            lax.all_gather(thin_rows[0], "tp", axis=0, tiled=True),
            lax.all_gather(thin_rows[1], "tp", axis=0, tiled=True),
            lax.all_gather(thin_rows[2], "tp", axis=0, tiled=True),
        )
        gate_flip, up_flip, down_flip = (sampler_mats[0], sampler_mats[1], sampler_mats[2])
        gates.append(gate_flip.T)
        ups.append(up_flip.T)
        downs.append(down_flip.T)

        def hidden_of(row_block):
            gate_act = lax.dot_general(
                row_block, gate_flip, contract_last, preferred_element_type=jnp.float32
            )
            up_act = lax.dot_general(
                row_block, up_flip, contract_last, preferred_element_type=jnp.float32
            )
            return (jax.nn.silu(gate_act) * up_act).astype(jnp.bfloat16)

        if section_idx == 0:
            hidden = hidden_of(normed)
        else:
            hidden = hidden_of(lax.all_gather(normed, "fs", axis=0, tiled=True))
        mixed = lax.psum_scatter(
            jnp.dot(hidden, down_flip, preferred_element_type=jnp.float32),
            "fs",
            scatter_dimension=0,
            tiled=True,
        )
        rounded_state = (residual + 0.5 * out_gain[section_idx] * normalize(mixed)).astype(
            jnp.bfloat16
        )
        if section_idx == 0:
            residual = rounded_state.astype(jnp.float32)
            normed = normalize(residual).astype(jnp.bfloat16)
    return (jnp.stack(gates), jnp.stack(ups), jnp.stack(downs), rounded_state)


ORDER = (0, 3, 1, 2)
TURNED = ((0, 1), (2, 1), (4, 1))
LAST = (((1,), (1,)), ((), ()))
MESH = pl.DeviceIdType.MESH


def cuts(extent, width):
    return [(start, min(width, extent - start)) for start in range(0, extent, width)]


def fused_kernel(tokens, gate_w, up_w, down_w, in_gain, out_gain, *refs):
    cols = gate_w.shape[2]
    full = [refs[0].at[pl.ds(m * cols, cols), :] for m in range(6)]
    state = refs[0]
    stage, flip, tok, normed, hidden, part, rin, lin, rout, lout, rs = refs[1:12]
    load_sem, tok_sem, send_sem, recv_sem = refs[12:]
    y, z, t = lax.axis_index("grp"), lax.axis_index("fs"), lax.axis_index("tp")
    x, c = t // 2, lax.rem(t, 2)
    other_y, other_x, other_c = 1 - y, (1 - x) * 2 + c, x * 2 + (1 - c)
    other_both = (1 - x) * 2 + (1 - c)
    groups = 4
    ahead, behind = lax.rem(z + 1, groups), lax.rem(z + groups - 1, groups)
    to_x, to_c, to_y = {"tp": other_x}, {"tp": other_c}, {"grp": other_y}
    to_right, to_left = {"fs": ahead}, {"fs": behind}
    _, rows, cols = gate_w.shape
    half_rows = rows // 2
    block = cols // groups
    half = block // 2
    count, width = tokens.shape
    quarter = count // groups
    piece = count // 8
    f32, bf16 = jnp.float32, jnp.bfloat16
    weights = (gate_w, up_w, down_w)

    names = []
    sent = []

    def slot(name):
        if name not in names:
            names.append(name)
        return names.index(name)

    def remote(name, source, target, device):
        k = slot(name)
        return pltpu.make_async_remote_copy(
            src_ref=source,
            dst_ref=target,
            send_sem=send_sem.at[k],
            recv_sem=recv_sem.at[k],
            device_id=device,
            device_id_type=MESH,
        )

    def send(name, source, target, device):
        copy = remote(name, source, target, device)
        copy.start()
        return copy

    def arrived(name, landed, device):
        remote(name, landed, landed, device).wait_recv()

    def slabs(start, extent, step, work):
        def one(i, carry):
            work(pl.ds(pl.multiple_of(start + i * step, step), step))
            return carry

        lax.fori_loop(0, extent // step, one, 0)

    def place(m, column, which, source):
        top = pl.multiple_of(column * block + which * half, 16)
        return full[m].at[pl.ds(top, half), pl.ds(pl.multiple_of(source * rows, 128), rows)]

    def blocks_of(m, column, source):
        top = pl.multiple_of(column * block, 16)
        return full[m].at[pl.ds(top, block), pl.ds(pl.multiple_of(source * rows, 128), rows)]

    def rows_of(m, column):
        return full[m].at[pl.ds(pl.multiple_of(column * block, 16), block), :]

    def origin(order):
        return (z + 1 - 2 * lax.rem(z, 2), 2 - z // 2, 3 * (1 - z // 2))[order - 1]

    def load(k):
        m, r = k // 2, k % 2
        return pltpu.make_async_copy(
            weights[m % 3].at[m // 3, pl.ds(r * half_rows, half_rows), :],
            stage.at[k % 2],
            load_sem.at[k % 2],
        )

    fetch = []
    for p, chunk in enumerate(ORDER):
        fetch.append(
            pltpu.make_async_copy(
                tokens.at[pl.ds(chunk * quarter, quarter), :],
                tok.at[pl.ds(p * quarter, quarter), :],
                tok_sem.at[p],
            )
        )
    load(0).start()
    load(1).start()
    for copy in fetch:
        copy.start()

    partners = [{"fs": lax.rem(z + shift, groups)} for shift in range(1, groups)]
    partners += [to_x, to_c, to_y]
    barrier = pltpu.get_barrier_semaphore()
    for partner in partners:
        pl.semaphore_signal(barrier, inc=1, device_id=partner, device_id_type=MESH)

    def prep(m):
        layer, which, s = m // 3, m % 3, m % 3
        if m >= 3:
            for copy in copies_z(m - 3):
                copy.wait_send()
        for r in range(2):
            k = 2 * m + r
            load(k).wait()
            lanes = slice(r * half_rows, (r + 1) * half_rows)

            def one(i, carry):
                cut = pl.ds(pl.multiple_of(i * 128, 128), 128)
                turned = stage[k % 2, :, cut].T
                if which < 2:
                    turned = turned * in_gain[layer : layer + 1, lanes]
                flip[s, cut, lanes] = turned.astype(bf16)
                return carry

            lax.fori_loop(0, cols // 128, one, 0)
            if k + 2 < 12:
                load(k + 2).start()
        mine = flip[s, pl.ds(pl.multiple_of(z * block, 16), block), :]
        top = pl.multiple_of(t * block, 16)
        full[m][pl.ds(top, block), pl.ds(pl.multiple_of(z * rows, 128), rows)] = mine

    def copies_z(m):
        base = [slot(("z", m, order)) for order in range(1, groups)][0]
        outer = 1 - (lax.rem(z, 3) + 1) // 2
        copies = []
        for order in range(1, groups):
            target = origin(order)
            top = pl.multiple_of(target * block + y * half, 16)
            landing = base if order == 1 else base + 1 + outer
            copies.append(
                pltpu.make_async_remote_copy(
                    src_ref=flip.at[m % 3, pl.ds(top, half), :],
                    dst_ref=place(m, t, y, z),
                    send_sem=send_sem.at[base + order - 1],
                    recv_sem=recv_sem.at[landing],
                    device_id={"fs": target},
                    device_id_type=MESH,
                )
            )
        return copies

    def send_z(m):
        for copy in copies_z(m):
            copy.start()

    def send_x(m):
        spot = blocks_of(m, t, z)
        sent.append(send(("x", m, 0), spot, spot, to_x))

    def on_z(m, shift):
        source = origin(shift)
        spot = place(m, t, y, source)
        arrived(("z", m, shift), spot, {"fs": source})
        sent.append(send(("x", m, shift), spot, spot, to_x))
        sent.append(send(("y", m, shift), spot, spot, to_y))

    def on_x(m, shift):
        spot = place(m, other_x, y, origin(shift))
        arrived(("x", m, shift), spot, to_x)
        sent.append(send(("w", m, shift), spot, spot, to_y))

    def turn(m, order):
        spot = place(m, t, other_y, origin(order))
        arrived(("y", m, order), spot, to_y)
        sent.append(send(("w", m, order), spot, spot, to_x))

    def share(m, far, order):
        spot = blocks_of(m, other_x if far else t, origin(order) if order else z)
        sent.append(send(("c", m, far, order), spot, spot, to_c))

    def finish(m):
        share(m, 0, 0)
        arrived(("x", m, 0), blocks_of(m, other_x, z), to_x)
        share(m, 1, 0)
        for order in range(1, groups):
            if (m, order) in TURNED:
                arrived(("x", m, order), place(m, other_x, y, origin(order)), to_x)
            else:
                arrived(("y", m, order), place(m, t, other_y, origin(order)), to_y)
            share(m, 0, order)
        for order in range(1, groups):
            device = to_x if (m, order) in TURNED else to_y
            arrived(("w", m, order), place(m, other_x, other_y, origin(order)), device)
            share(m, 1, order)

    def on_c(m):
        for far, column in ((0, other_c), (1, other_both)):
            for order in range(groups):
                spot = blocks_of(m, column, origin(order) if order else z)
                arrived(("c", m, far, order), spot, to_c)

    def scaled(value):
        return value * lax.rsqrt(jnp.mean(value * value, axis=-1, keepdims=True) + EPS)

    def gated(layer, start, extent, cut):
        first, size = cut
        line = normed[start : start + extent, :]
        gate = lax.dot_general(
            line, full[3 * layer][first : first + size, :], LAST, preferred_element_type=f32
        )
        lift = lax.dot_general(
            line, full[3 * layer + 1][first : first + size, :], LAST, preferred_element_type=f32
        )
        value = jax.nn.silu(gate) * lift
        hidden[start : start + extent, first : first + size] = value.astype(bf16)

    def summed(layer, start, extent):
        line = hidden[start : start + extent, :]
        for first, size in cuts(width, 512):
            part[start : start + extent, first : first + size] = jnp.dot(
                line, full[3 * layer + 2][:, first : first + size], preferred_element_type=f32
            ).astype(bf16)

    def add_into(target, landed, offset, start, extent):
        def work(line):
            other = landed[line, :] if offset is None else landed[offset, line, :]
            total = other.astype(f32) + part[line, :].astype(f32)
            target[line, :] = total.astype(bf16)

        slabs(start, extent, 32, work)

    def lines(j):
        return pl.ds(j * piece, piece)

    def pass_right(j):
        arrived(("R", j), rin.at[lines(j), :], to_left)
        add_into(rout, rin, None, j * piece, piece)
        send(("R", j), rout.at[lines(j), :], rin.at[lines(j), :], to_right)

    def pass_left(j):
        arrived(("L", j), lin.at[lines(j), :], to_right)
        add_into(lout, lin, None, j * piece, piece)
        send(("L", j), lout.at[lines(j), :], lin.at[lines(j), :], to_left)

    def near(j):
        @pl.when(z == 1)
        def _():
            pass_right(j)

        @pl.when(z == 2)
        def _():
            pass_left(j)

    def edge(j):
        @pl.when(z == 0)
        def _():
            send(("R", j), part.at[lines(j), :], rin.at[lines(j), :], to_right)

        @pl.when(z == groups - 1)
        def _():
            send(("L", j), part.at[lines(j), :], lin.at[lines(j), :], to_left)

    def far(j):
        @pl.when(z == 1)
        def _():
            pass_left(j)

        @pl.when(z == 2)
        def _():
            pass_right(j)

    def settle(j):
        @pl.when(z == 0)
        def _():
            arrived(("L", j), lin.at[lines(j), :], to_right)

        @pl.when(z == groups - 1)
        def _():
            arrived(("R", j), rin.at[lines(j), :], to_left)

        def work(line):
            total = part[line, :].astype(f32) + rin[line, :].astype(f32) + lin[line, :].astype(f32)
            after = tok[line, :].astype(f32) + 0.5 * out_gain[0:1, :] * scaled(total)
            after = after.astype(bf16)
            tok[line, :] = after
            normed[line, :] = scaled(after.astype(f32)).astype(bf16)

        slabs(j * piece, piece, 32, work)

    def exchange(i):
        if i < 8:
            near(i)
        if 0 <= i - 1 < 8:
            far(i - 1)
        if 0 <= i - 3 < 8:
            settle(i - 3)

    def exchange_sent(first, last):
        for j in range(first, last):

            @pl.when(z < groups - 1)
            def _():
                remote(("R", j), rout.at[lines(j), :], rin.at[lines(j), :], to_right).wait_send()

            @pl.when(z > 0)
            def _():
                remote(("L", j), lout.at[lines(j), :], lin.at[lines(j), :], to_left).wait_send()

    def parts_of(k):
        return [j for j in range(8) if ORDER[j // 2] == k]

    def reduce_edge(rightward, leftward):
        @pl.when(z == 0)
        def _():
            for j in parts_of(rightward):
                send(("r", j), part.at[lines(j), :], rs.at[lines(j), :], to_right)

        @pl.when(z == groups - 1)
        def _():
            for j in parts_of(leftward):
                send(("l", j), part.at[lines(j), :], rs.at[lines(j), :], to_left)

    def reduce_right(j):
        arrived(("r", j), rs.at[lines(j), :], to_left)
        add_into(rout, rs, None, j * piece, piece)
        send(("r", j), rout.at[lines(j), :], rs.at[lines(j), :], to_right)

    def reduce_left(j):
        arrived(("l", j), rs.at[lines(j), :], to_right)
        add_into(lout, rs, None, j * piece, piece)
        send(("l", j), lout.at[lines(j), :], rs.at[lines(j), :], to_left)

    def reduce_all():
        for j in range(2):

            @pl.when(z == 1)
            def _():
                reduce_right(parts_of(3)[j])

            @pl.when(z == 2)
            def _():
                reduce_left(parts_of(0)[j])

    def leave(row, line, value):
        state[pl.ds(line.start + row, 32), :] = value

    def conclude():
        base = 6 * cols
        for k in range(groups):
            start = ORDER.index(k) * quarter

            @pl.when(z == k)
            def _():
                def keep(line):
                    leave(base + 2 * quarter - start, line, part[line, :])
                    leave(base + 3 * quarter - start, line, tok[line, :])

                slabs(start, quarter, 32, keep)

        for j in range(2):
            for k in range(1, groups):
                ahead_j = parts_of(k)[j]
                shift = base - ORDER.index(k) * quarter

                @pl.when(z == k - 1)
                def _():
                    if k > 1:
                        arrived(("r", ahead_j), rs.at[lines(ahead_j), :], to_left)

                    def work(line):
                        total = part[line, :].astype(f32)
                        if k > 1:
                            total += rs[line, :].astype(f32)
                        leave(shift, line, total.astype(bf16))

                    slabs(ahead_j * piece, piece, 32, work)

            for k in reversed(range(groups - 1)):
                back_j = parts_of(k)[j]
                shift = base + quarter - ORDER.index(k) * quarter

                @pl.when(z == k + 1)
                def _():
                    if k < groups - 2:
                        arrived(("l", back_j), rs.at[lines(back_j), :], to_right)

                    def work(line):
                        total = part[line, :].astype(f32)
                        if k < groups - 2:
                            total += rs[line, :].astype(f32)
                        leave(shift, line, total.astype(bf16))

                    slabs(back_j * piece, piece, 32, work)

        for k in (2, 3):
            for j in parts_of(k):

                @pl.when(z < k - 1)
                def _():
                    remote(("r", j), rout.at[lines(j), :], rs.at[lines(j), :], to_right).wait_send()

        for k in (0, 1):
            for j in parts_of(k):

                @pl.when(z > k + 1)
                def _():
                    remote(("l", j), lout.at[lines(j), :], rs.at[lines(j), :], to_left).wait_send()

    prep(0)
    pl.semaphore_wait(barrier, len(partners))
    send_z(0)
    send_x(0)
    prep(1)
    prep(2)
    for copy in fetch:
        copy.wait()

    def first_norm(line):
        normed[line, :] = scaled(tok[line, :].astype(f32)).astype(bf16)

    on_z(0, 1)
    slabs(0, count, 32, first_norm)

    @pl.when(z == 0)
    def _():
        rin[...] = jnp.zeros_like(rin)

    @pl.when(z == groups - 1)
    def _():
        lin[...] = jnp.zeros_like(lin)

    pieces = cuts(cols, 384)
    whole = (0, count)
    upper, lower = (0, count // 2), (count // 2, count // 2)

    on_z(0, 2)
    send_z(1)
    turn(0, 1)
    on_z(0, 3)
    on_x(0, 2)
    on_x(0, 3)
    on_z(1, 1)
    on_z(1, 2)
    send_z(2)
    finish(0)
    on_x(1, 1)
    on_z(1, 3)
    send_x(1)
    on_x(1, 2)
    on_x(1, 3)
    on_z(2, 1)
    prep(3)
    on_z(2, 2)
    send_z(3)
    on_z(2, 3)
    prep(4)
    send_z(4)
    on_x(2, 2)
    finish(1)
    on_x(2, 3)
    turn(2, 1)
    send_x(2)
    on_z(3, 1)
    prep(5)
    on_c(0)
    on_c(1)
    gated(0, *whole, pieces[0])
    on_z(3, 2)
    send_z(5)
    gated(0, *whole, pieces[1])
    on_z(3, 3)
    gated(0, *whole, pieces[2])
    on_x(3, 1)
    gated(0, *whole, pieces[3])
    finish(2)
    on_x(3, 2)
    send_x(3)
    on_c(2)
    summed(0, *upper)
    for j in range(4):
        edge(j)
    summed(0, *lower)
    for j in range(4, 8):
        edge(j)
    on_x(3, 3)
    on_z(4, 1)
    on_z(4, 2)
    on_z(4, 3)
    exchange(0)
    finish(3)
    exchange(1)
    turn(4, 1)
    on_x(4, 2)
    exchange(2)
    on_x(4, 3)
    send_x(4)
    on_z(5, 1)
    on_z(5, 2)
    exchange(3)
    on_x(5, 1)
    on_z(5, 3)
    exchange(4)
    finish(4)
    send_x(5)
    exchange(5)
    on_x(5, 2)
    exchange(6)
    on_x(5, 3)
    on_c(3)
    on_c(4)
    for cut in pieces:
        gated(1, *upper, cut)
    exchange(7)
    finish(5)
    exchange(8)
    on_c(5)
    exchange_sent(0, 4)
    summed(1, *upper)
    reduce_edge(3, 0)
    exchange(9)
    exchange(10)
    for cut in pieces:
        gated(1, *lower, cut)
    exchange_sent(4, 8)
    summed(1, *lower)
    reduce_edge(2, 1)
    reduce_all()
    conclude()
    for m in (3, 4, 5):
        sent.extend(copies_z(m))
    for copy in sent:
        copy.wait_send()


def fused(tokens, gate_weight, up_weight, down_weight, in_gain, out_gain):
    count, width = tokens.shape
    _, rows, cols = gate_weight.shape
    bf16 = jnp.bfloat16
    quarter = count // 4
    whole = pl.BlockSpec(memory_space=pl.ANY)
    near = pl.BlockSpec(memory_space=pltpu.VMEM)
    band = pltpu.VMEM((count, width), bf16)
    messages = 160
    return pl.pallas_call(
        fused_kernel,
        in_specs=[whole] * 4 + [near] * 2,
        out_specs=near,
        out_shape=pltpu.VMEM((6 * cols + count, width), bf16),
        scratch_shapes=[
            pltpu.VMEM((2, rows // 2, cols), jnp.float32),
            pltpu.VMEM((3, cols, rows), bf16),
            band,
            band,
            pltpu.VMEM((count, cols), bf16),
            band,
            band,
            band,
            band,
            band,
            band,
            pltpu.SemaphoreType.DMA((2,)),
            pltpu.SemaphoreType.DMA((4,)),
            pltpu.SemaphoreType.DMA((messages,)),
            pltpu.SemaphoreType.DMA((messages,)),
        ],
        compiler_params=pltpu.CompilerParams(
            collective_id=0, has_side_effects=True, vmem_limit_bytes=27 * 2**20
        ),
    )(tokens, gate_weight, up_weight, down_weight, in_gain, out_gain)


def emit_kernel(flips, *refs):
    outs, (held, sems) = refs[:3], refs[3:]
    slots, step, cols = held.shape
    width = flips.shape[1]
    steps = width // step

    def out_copy(k, i):
        slot = lax.rem(i, slots)
        top = pl.multiple_of(i * step, step)
        return pltpu.make_async_copy(
            held.at[slot], outs[k % 3].at[k // 3, pl.ds(top, step), :], sems.at[slot]
        )

    for k in range(6):

        def one(i, carry):
            if k == 0:

                @pl.when(i >= slots)
                def _():
                    out_copy(k, i).wait()

            else:
                out_copy(k, i).wait()
            lanes = pl.ds(pl.multiple_of(i * step, step), step)
            held[lax.rem(i, slots)] = flips[k * cols : (k + 1) * cols, lanes].T
            out_copy(k, i).start()
            return carry

        lax.fori_loop(0, steps, one, 0)
    for i in range(slots):
        out_copy(5, steps - slots + i).wait()


def emit(flips, cols):
    width = flips.shape[1]
    near = pl.BlockSpec(memory_space=pltpu.VMEM)
    whole = pl.BlockSpec(memory_space=pl.ANY)
    return pl.pallas_call(
        emit_kernel,
        in_specs=[near],
        out_specs=[whole] * 3,
        out_shape=[jax.ShapeDtypeStruct((2, width, cols), jnp.bfloat16)] * 3,
        scratch_shapes=[
            pltpu.VMEM((8, 256, cols), jnp.bfloat16),
            pltpu.SemaphoreType.DMA((8,)),
        ],
        compiler_params=pltpu.CompilerParams(vmem_limit_bytes=8 * 2**20),
        cost_estimate=pl.CostEstimate(
            flops=10**10, bytes_accessed=12 * cols * width, transcendentals=0
        ),
    )(flips)


def last_kernel(rest, left, right, out_gain, result):
    quarter = result.shape[0]

    def one(i, carry):
        line = pl.ds(pl.multiple_of(i * 32, 32), 32)
        total = rest[line, :].astype(jnp.float32) + left[line, :].astype(jnp.float32)
        total += right[line, :].astype(jnp.float32)
        before = rest[pl.ds(pl.multiple_of(quarter + i * 32, 32), 32), :].astype(jnp.float32)
        after = before + 0.5 * out_gain[1:2, :] * normalize(total)
        result[line, :] = after.astype(jnp.bfloat16)
        return carry

    lax.fori_loop(0, quarter // 32, one, 0)


def last_step(rest, left, right, out_gain):
    near = pl.BlockSpec(memory_space=pltpu.VMEM)
    return pl.pallas_call(
        last_kernel,
        in_specs=[near] * 4,
        out_specs=near,
        out_shape=jax.ShapeDtypeStruct(left.shape, jnp.bfloat16),
        compiler_params=pltpu.CompilerParams(vmem_limit_bytes=8 * 2**20),
    )(rest, left, right, out_gain)


def body(tokens, gate_weight, up_weight, down_weight, in_gain, out_gain):
    groups, halves = lax.axis_size("fs"), lax.axis_size("grp")
    columns = lax.axis_size("tp")
    count, model_width = tokens.shape
    _, rows, cols = gate_weight.shape
    odd = cols % (32 * groups) or rows % 256 or cols % 128 or count % 512 or model_width % 2048
    if odd or halves != 2 or columns != 4 or groups != 4:
        return body_plain(tokens, gate_weight, up_weight, down_weight, in_gain, out_gain)
    flips = fused(tokens, gate_weight, up_weight, down_weight, in_gain, out_gain)
    quarter = count // groups
    base = 6 * cols
    ahead = lax.slice_in_dim(flips, base, base + quarter)
    back = lax.slice_in_dim(flips, base + quarter, base + 2 * quarter)
    rest = lax.slice_in_dim(flips, base + 2 * quarter, base + 4 * quarter)
    left = lax.ppermute(ahead, "fs", [(i, i + 1) for i in range(groups - 1)])
    right = lax.ppermute(back, "fs", [(i + 1, i) for i in range(groups - 1)])
    outs = emit(flips, cols)
    return (*outs, last_step(rest, left, right, out_gain))


def solution(mesh):
    in_specs = (
        P(("grp", "tp"), None),
        P(None, "fs", "tp"),
        P(None, "fs", "tp"),
        P(None, "fs", "tp"),
        P(None, "fs"),
        P(),
    )
    out_specs = (
        P("grp", None, "fs"),
        P("grp", None, "fs"),
        P("grp", None, "fs"),
        P(("grp", "tp", "fs"), None),
    )
    return jax.shard_map(body, mesh=mesh, in_specs=in_specs, out_specs=out_specs, check_vma=False)
```

```python
import functools

import jax
import jax.numpy as jnp
from jax import lax
from jax.experimental import pallas as pl
from jax.experimental.pallas import tpu as pltpu
from jax.sharding import PartitionSpec as P

EPS = 1e-06


def normalize(rows):
    return rows * lax.rsqrt(jnp.mean(rows * rows, axis=-1, keepdims=True) + EPS)


def body_plain(tokens, gate_weight, up_weight, down_weight, in_gain, out_gain):
    groups = lax.axis_size("fs")
    rows_all = tokens.shape[0]
    rows_mine = rows_all // groups
    model_width = tokens.shape[1]
    local_rows = gate_weight.shape[1]
    block_width = gate_weight.shape[2] // groups
    residual = lax.dynamic_slice_in_dim(
        tokens, lax.axis_index("fs") * rows_mine, rows_mine, 0
    ).astype(jnp.float32)
    normed = normalize(tokens.astype(jnp.float32)).astype(jnp.bfloat16)
    gates = []
    ups = []
    downs = []
    rounded_state = tokens
    contract_last = (((1,), (1,)), ((), ()))
    for section_idx in range(2):
        scale = in_gain[section_idx][:, None]
        gate_rounded = (scale * gate_weight[section_idx]).astype(jnp.bfloat16)
        up_rounded = (scale * up_weight[section_idx]).astype(jnp.bfloat16)
        down_rounded = down_weight[section_idx].astype(jnp.bfloat16)
        flipped = [
            w.T.reshape(groups, block_width, local_rows)
            for w in (gate_rounded, up_rounded, down_rounded)
        ]
        arrived = (
            lax.all_to_all(flipped[0], "fs", split_axis=0, concat_axis=2, tiled=True),
            lax.all_to_all(flipped[1], "fs", split_axis=0, concat_axis=2, tiled=True),
            lax.all_to_all(flipped[2], "fs", split_axis=0, concat_axis=2, tiled=True),
        )
        thin_rows = [w.reshape(block_width, model_width) for w in arrived]
        sampler_mats = (
            lax.all_gather(thin_rows[0], "tp", axis=0, tiled=True),
            lax.all_gather(thin_rows[1], "tp", axis=0, tiled=True),
            lax.all_gather(thin_rows[2], "tp", axis=0, tiled=True),
        )
        gate_flip, up_flip, down_flip = (sampler_mats[0], sampler_mats[1], sampler_mats[2])
        gates.append(gate_flip.T)
        ups.append(up_flip.T)
        downs.append(down_flip.T)

        def hidden_of(row_block):
            gate_act = lax.dot_general(
                row_block, gate_flip, contract_last, preferred_element_type=jnp.float32
            )
            up_act = lax.dot_general(
                row_block, up_flip, contract_last, preferred_element_type=jnp.float32
            )
            return (jax.nn.silu(gate_act) * up_act).astype(jnp.bfloat16)

        if section_idx == 0:
            hidden = hidden_of(normed)
        else:
            hidden = hidden_of(lax.all_gather(normed, "fs", axis=0, tiled=True))
        mixed = lax.psum_scatter(
            jnp.dot(hidden, down_flip, preferred_element_type=jnp.float32),
            "fs",
            scatter_dimension=0,
            tiled=True,
        )
        rounded_state = (residual + 0.5 * out_gain[section_idx] * normalize(mixed)).astype(
            jnp.bfloat16
        )
        if section_idx == 0:
            residual = rounded_state.astype(jnp.float32)
            normed = normalize(residual).astype(jnp.bfloat16)
    return (jnp.stack(gates), jnp.stack(ups), jnp.stack(downs), rounded_state)


ORDER = (0, 3, 1, 2)
TURNED = ((0, 1), (2, 1), (4, 1))
LAST = (((1,), (1,)), ((), ()))
MESH = pl.DeviceIdType.MESH


def cuts(extent, width):
    return [(start, min(width, extent - start)) for start in range(0, extent, width)]


def fused_kernel(tokens, gate_w, up_w, down_w, in_gain, out_gain, *refs):
    cols = gate_w.shape[2]
    full = [refs[0].at[pl.ds(m * cols, cols), :] for m in range(6)]
    state = refs[0]
    stage, flip, tok, normed, hidden, part, rin, lin, rout, lout, rs = refs[1:12]
    load_sem, tok_sem, send_sem, recv_sem = refs[12:]
    y, z, t = lax.axis_index("grp"), lax.axis_index("fs"), lax.axis_index("tp")
    x, c = t // 2, lax.rem(t, 2)
    other_y, other_x, other_c = 1 - y, (1 - x) * 2 + c, x * 2 + (1 - c)
    other_both = (1 - x) * 2 + (1 - c)
    groups = 4
    ahead, behind = lax.rem(z + 1, groups), lax.rem(z + groups - 1, groups)
    to_x, to_c, to_y = {"tp": other_x}, {"tp": other_c}, {"grp": other_y}
    to_right, to_left = {"fs": ahead}, {"fs": behind}
    _, rows, cols = gate_w.shape
    half_rows = rows // 2
    block = cols // groups
    half = block // 2
    count, width = tokens.shape
    quarter = count // groups
    piece = count // 8
    f32, bf16 = jnp.float32, jnp.bfloat16
    weights = (gate_w, up_w, down_w)

    names = []
    sent = []

    def slot(name):
        if name not in names:
            names.append(name)
        return names.index(name)

    def remote(name, source, target, device):
        k = slot(name)
        return pltpu.make_async_remote_copy(
            src_ref=source,
            dst_ref=target,
            send_sem=send_sem.at[k],
            recv_sem=recv_sem.at[k],
            device_id=device,
            device_id_type=MESH,
        )

    def send(name, source, target, device):
        copy = remote(name, source, target, device)
        copy.start()
        return copy

    def arrived(name, landed, device):
        remote(name, landed, landed, device).wait_recv()

    def slabs(start, extent, step, work):
        def one(i, carry):
            work(pl.ds(pl.multiple_of(start + i * step, step), step))
            return carry

        lax.fori_loop(0, extent // step, one, 0)

    def place(m, column, which, source):
        top = pl.multiple_of(column * block + which * half, 16)
        return full[m].at[pl.ds(top, half), pl.ds(pl.multiple_of(source * rows, 128), rows)]

    def blocks_of(m, column, source):
        top = pl.multiple_of(column * block, 16)
        return full[m].at[pl.ds(top, block), pl.ds(pl.multiple_of(source * rows, 128), rows)]

    def rows_of(m, column):
        return full[m].at[pl.ds(pl.multiple_of(column * block, 16), block), :]

    def origin(order):
        return (z + 1 - 2 * lax.rem(z, 2), 2 - z // 2, 3 * (1 - z // 2))[order - 1]

    def load(k):
        m, r = k // 2, k % 2
        return pltpu.make_async_copy(
            weights[m % 3].at[m // 3, pl.ds(r * half_rows, half_rows), :],
            stage.at[k % 2],
            load_sem.at[k % 2],
        )

    fetch = []
    for p, chunk in enumerate(ORDER):
        fetch.append(
            pltpu.make_async_copy(
                tokens.at[pl.ds(chunk * quarter, quarter), :],
                tok.at[pl.ds(p * quarter, quarter), :],
                tok_sem.at[p],
            )
        )
    load(0).start()
    load(1).start()

    partners = [{"fs": lax.rem(z + shift, groups)} for shift in range(1, groups)]
    partners += [to_x, to_c, to_y]
    barrier = pltpu.get_barrier_semaphore()
    for partner in partners:
        pl.semaphore_signal(barrier, inc=1, device_id=partner, device_id_type=MESH)

    def prep(m, after=None):
        layer, which, s = m // 3, m % 3, m % 3
        if m >= 3:
            for copy in all_z(m - 3):
                copy.wait_send()
        for r in range(2):
            k = 2 * m + r
            load(k).wait()
            lanes = slice(r * half_rows, (r + 1) * half_rows)

            def one(i, carry):
                cut = pl.ds(pl.multiple_of(i * 128, 128), 128)
                turned = stage[k % 2, :, cut].T
                if which < 2:
                    turned = turned * in_gain[layer : layer + 1, lanes]
                flip[s, cut, lanes] = turned.astype(bf16)
                return carry

            lax.fori_loop(0, cols // 128, one, 0)
            if after is not None:
                after(r)
            if k + 2 < 12:
                load(k + 2).start()
        mine = flip[s, pl.ds(pl.multiple_of(z * block, 16), block), :]
        top = pl.multiple_of(t * block, 16)
        full[m][pl.ds(top, block), pl.ds(pl.multiple_of(z * rows, 128), rows)] = mine

    def copies_z(m, part_of=None):
        kind = "z" if part_of is None else ("z0", "z1")[part_of]
        base = [slot((kind, m, order)) for order in range(1, groups)][0]
        first, size = (0, rows) if part_of is None else (part_of * half_rows, half_rows)
        lanes = pl.ds(pl.multiple_of(z * rows + first, 128), size)
        spot = full[m].at[pl.ds(pl.multiple_of(t * block + y * half, 16), half), lanes]
        late = 1 - (lax.rem(z, 3) + 1) // 2
        copies = []
        for order in range(1, groups):
            target = origin(order)
            top = pl.multiple_of(target * block + y * half, 16)
            landing = base if order == 1 else base + 1 + late
            copies.append(
                pltpu.make_async_remote_copy(
                    src_ref=flip.at[m % 3, pl.ds(top, half), pl.ds(first, size)],
                    dst_ref=spot,
                    send_sem=send_sem.at[base + order - 1],
                    recv_sem=recv_sem.at[landing],
                    device_id={"fs": target},
                    device_id_type=MESH,
                )
            )
        return copies

    def all_z(m):
        return copies_z(0, 0) + copies_z(0, 1) if m == 0 else copies_z(m)

    def send_z(m):
        for copy in copies_z(m):
            copy.start()

    def own_x(m):
        spot = blocks_of(m, t, z)
        return remote(("x", m, 0), spot, spot, to_x)

    def send_x(m):
        own_x(m).start()
        sent.append(own_x(m))

    def on_z(m, shift):
        source = origin(shift)
        spot = place(m, t, y, source)
        if m == 0:
            top = pl.multiple_of(t * block + y * half, 16)
            for r in range(2):
                lanes = pl.ds(pl.multiple_of(source * rows + r * half_rows, 128), half_rows)
                landed = full[m].at[pl.ds(top, half), lanes]
                arrived((("z0", "z1")[r], m, shift), landed, {"fs": source})
        else:
            arrived(("z", m, shift), spot, {"fs": source})
        sent.append(send(("x", m, shift), spot, spot, to_x))
        sent.append(send(("y", m, shift), spot, spot, to_y))

    def on_x(m, shift):
        spot = place(m, other_x, y, origin(shift))
        arrived(("x", m, shift), spot, to_x)
        sent.append(send(("w", m, shift), spot, spot, to_y))

    def turn(m, order):
        spot = place(m, t, other_y, origin(order))
        arrived(("y", m, order), spot, to_y)
        sent.append(send(("w", m, order), spot, spot, to_x))

    def share(m, far, order):
        spot = blocks_of(m, other_x if far else t, origin(order) if order else z)
        sent.append(send(("c", m, far, order), spot, spot, to_c))

    def finish(m):
        share(m, 0, 0)
        arrived(("x", m, 0), blocks_of(m, other_x, z), to_x)
        share(m, 1, 0)
        for order in range(1, groups):
            if (m, order) in TURNED:
                arrived(("x", m, order), place(m, other_x, y, origin(order)), to_x)
            else:
                arrived(("y", m, order), place(m, t, other_y, origin(order)), to_y)
            share(m, 0, order)
        for order in range(1, groups):
            device = to_x if (m, order) in TURNED else to_y
            arrived(("w", m, order), place(m, other_x, other_y, origin(order)), device)
            share(m, 1, order)

    def on_c(m):
        for far, column in ((0, other_c), (1, other_both)):
            for order in range(groups):
                spot = blocks_of(m, column, origin(order) if order else z)
                arrived(("c", m, far, order), spot, to_c)

    def scaled(value):
        return value * lax.rsqrt(jnp.mean(value * value, axis=-1, keepdims=True) + EPS)

    def gated(layer, start, extent, cut):
        first, size = cut
        line = normed[start : start + extent, :]
        gate = lax.dot_general(
            line, full[3 * layer][first : first + size, :], LAST, preferred_element_type=f32
        )
        lift = lax.dot_general(
            line, full[3 * layer + 1][first : first + size, :], LAST, preferred_element_type=f32
        )
        value = jax.nn.silu(gate) * lift
        hidden[start : start + extent, first : first + size] = value.astype(bf16)

    def summed(layer, start, extent):
        line = hidden[start : start + extent, :]
        for first, size in cuts(width, 512):
            part[start : start + extent, first : first + size] = jnp.dot(
                line, full[3 * layer + 2][:, first : first + size], preferred_element_type=f32
            ).astype(bf16)

    def add_into(target, landed, offset, start, extent):
        def work(line):
            other = landed[line, :] if offset is None else landed[offset, line, :]
            total = other.astype(f32) + part[line, :].astype(f32)
            target[line, :] = total.astype(bf16)

        slabs(start, extent, 32, work)

    def lines(j):
        return pl.ds(j * piece, piece)

    def pass_right(j):
        arrived(("R", j), rin.at[lines(j), :], to_left)
        add_into(rout, rin, None, j * piece, piece)
        send(("R", j), rout.at[lines(j), :], rin.at[lines(j), :], to_right)

    def pass_left(j):
        arrived(("L", j), lin.at[lines(j), :], to_right)
        add_into(lout, lin, None, j * piece, piece)
        send(("L", j), lout.at[lines(j), :], lin.at[lines(j), :], to_left)

    def near(j):
        @pl.when(z == 1)
        def _():
            pass_right(j)

        @pl.when(z == 2)
        def _():
            pass_left(j)

    def edge(j):
        @pl.when(z == 0)
        def _():
            send(("R", j), part.at[lines(j), :], rin.at[lines(j), :], to_right)

        @pl.when(z == groups - 1)
        def _():
            send(("L", j), part.at[lines(j), :], lin.at[lines(j), :], to_left)

    def far(j):
        @pl.when(z == 1)
        def _():
            pass_left(j)

        @pl.when(z == 2)
        def _():
            pass_right(j)

    def settle(j):
        @pl.when(z == 0)
        def _():
            arrived(("L", j), lin.at[lines(j), :], to_right)

        @pl.when(z == groups - 1)
        def _():
            arrived(("R", j), rin.at[lines(j), :], to_left)

        def work(line):
            total = part[line, :].astype(f32) + rin[line, :].astype(f32) + lin[line, :].astype(f32)
            after = tok[line, :].astype(f32) + 0.5 * out_gain[0:1, :] * scaled(total)
            after = after.astype(bf16)
            tok[line, :] = after
            normed[line, :] = scaled(after.astype(f32)).astype(bf16)

        slabs(j * piece, piece, 32, work)

    def exchange(i):
        if i < 8:
            near(i)
        if 0 <= i - 1 < 8:
            far(i - 1)
        if 0 <= i - 3 < 8:
            settle(i - 3)

    def exchange_sent(first, last):
        for j in range(first, last):

            @pl.when(z < groups - 1)
            def _():
                remote(("R", j), rout.at[lines(j), :], rin.at[lines(j), :], to_right).wait_send()

            @pl.when(z > 0)
            def _():
                remote(("L", j), lout.at[lines(j), :], lin.at[lines(j), :], to_left).wait_send()

    def parts_of(k):
        return [j for j in range(8) if ORDER[j // 2] == k]

    def reduce_edge(rightward, leftward):
        @pl.when(z == 0)
        def _():
            for j in parts_of(rightward):
                send(("r", j), part.at[lines(j), :], rs.at[lines(j), :], to_right)

        @pl.when(z == groups - 1)
        def _():
            for j in parts_of(leftward):
                send(("l", j), part.at[lines(j), :], rs.at[lines(j), :], to_left)

    def reduce_right(j):
        arrived(("r", j), rs.at[lines(j), :], to_left)
        add_into(rout, rs, None, j * piece, piece)
        send(("r", j), rout.at[lines(j), :], rs.at[lines(j), :], to_right)

    def reduce_left(j):
        arrived(("l", j), rs.at[lines(j), :], to_right)
        add_into(lout, rs, None, j * piece, piece)
        send(("l", j), lout.at[lines(j), :], rs.at[lines(j), :], to_left)

    def reduce_all():
        for j in range(2):

            @pl.when(z == 1)
            def _():
                reduce_right(parts_of(3)[j])

            @pl.when(z == 2)
            def _():
                reduce_left(parts_of(0)[j])

    def leave(row, line, value):
        state[pl.ds(line.start + row, 32), :] = value

    def conclude():
        base = 6 * cols
        for k in range(groups):
            start = ORDER.index(k) * quarter

            @pl.when(z == k)
            def _():
                def keep(line):
                    leave(base + 2 * quarter - start, line, part[line, :])
                    leave(base + 3 * quarter - start, line, tok[line, :])

                slabs(start, quarter, 32, keep)

        for j in range(2):
            for k in range(1, groups):
                ahead_j = parts_of(k)[j]
                shift = base - ORDER.index(k) * quarter

                @pl.when(z == k - 1)
                def _():
                    if k > 1:
                        arrived(("r", ahead_j), rs.at[lines(ahead_j), :], to_left)

                    def work(line):
                        total = part[line, :].astype(f32)
                        if k > 1:
                            total += rs[line, :].astype(f32)
                        leave(shift, line, total.astype(bf16))

                    slabs(ahead_j * piece, piece, 32, work)

            for k in reversed(range(groups - 1)):
                back_j = parts_of(k)[j]
                shift = base + quarter - ORDER.index(k) * quarter

                @pl.when(z == k + 1)
                def _():
                    if k < groups - 2:
                        arrived(("l", back_j), rs.at[lines(back_j), :], to_right)

                    def work(line):
                        total = part[line, :].astype(f32)
                        if k < groups - 2:
                            total += rs[line, :].astype(f32)
                        leave(shift, line, total.astype(bf16))

                    slabs(back_j * piece, piece, 32, work)

        for k in (2, 3):
            for j in parts_of(k):

                @pl.when(z < k - 1)
                def _():
                    remote(("r", j), rout.at[lines(j), :], rs.at[lines(j), :], to_right).wait_send()

        for k in (0, 1):
            for j in parts_of(k):

                @pl.when(z > k + 1)
                def _():
                    remote(("l", j), lout.at[lines(j), :], rs.at[lines(j), :], to_left).wait_send()

    def early(r):
        if r == 0:
            pl.semaphore_wait(barrier, len(partners))
        for copy in copies_z(0, r):
            copy.start()

    prep(0, early)
    send_x(0)
    for copy in fetch:
        copy.start()
    prep(1)
    prep(2)
    for copy in fetch:
        copy.wait()

    def first_norm(line):
        normed[line, :] = scaled(tok[line, :].astype(f32)).astype(bf16)

    on_z(0, 1)
    slabs(0, count, 32, first_norm)

    @pl.when(z == 0)
    def _():
        rin[...] = jnp.zeros_like(rin)

    @pl.when(z == groups - 1)
    def _():
        lin[...] = jnp.zeros_like(lin)

    pieces = cuts(cols, 384)
    whole = (0, count)
    upper, lower = (0, count // 2), (count // 2, count // 2)

    on_z(0, 2)
    send_z(1)
    turn(0, 1)
    on_z(0, 3)
    on_x(0, 2)
    on_x(0, 3)
    on_z(1, 1)
    on_z(1, 2)
    send_z(2)
    finish(0)
    on_x(1, 1)
    on_z(1, 3)
    send_x(1)
    on_x(1, 2)
    on_x(1, 3)
    on_z(2, 1)
    prep(3)
    on_z(2, 2)
    send_z(3)
    on_z(2, 3)
    prep(4)
    send_z(4)
    on_x(2, 2)
    finish(1)
    on_x(2, 3)
    turn(2, 1)
    send_x(2)
    on_z(3, 1)
    prep(5)
    on_c(0)
    on_c(1)
    gated(0, *whole, pieces[0])
    on_z(3, 2)
    send_z(5)
    gated(0, *whole, pieces[1])
    on_z(3, 3)
    gated(0, *whole, pieces[2])
    gated(0, *whole, pieces[3])
    finish(2)
    on_x(3, 1)
    send_x(3)
    on_c(2)
    summed(0, *upper)
    for j in range(4):
        edge(j)
    summed(0, *lower)
    for j in range(4, 8):
        edge(j)
    on_x(3, 2)
    on_z(4, 1)
    on_z(4, 2)
    on_x(3, 3)
    on_z(4, 3)
    send_x(4)
    exchange(0)
    exchange(1)
    turn(4, 1)
    on_x(4, 2)
    exchange(2)
    on_z(5, 1)
    on_z(5, 2)
    on_x(4, 3)
    on_z(5, 3)
    send_x(5)
    exchange(3)
    finish(3)
    exchange(4)
    on_x(5, 1)
    finish(4)
    exchange(5)
    on_x(5, 2)
    exchange(6)
    on_x(5, 3)
    on_c(3)
    on_c(4)
    for cut in pieces:
        gated(1, *upper, cut)
    exchange(7)
    finish(5)
    exchange(8)
    on_c(5)
    exchange_sent(0, 4)
    summed(1, *upper)
    reduce_edge(3, 0)
    exchange(9)
    exchange(10)
    for cut in pieces:
        gated(1, *lower, cut)
    exchange_sent(4, 8)
    summed(1, *lower)
    reduce_edge(2, 1)
    reduce_all()
    conclude()
    for m in (3, 4, 5):
        sent.extend(copies_z(m))
    for copy in sent:
        copy.wait_send()


def fused(tokens, gate_weight, up_weight, down_weight, in_gain, out_gain):
    count, width = tokens.shape
    _, rows, cols = gate_weight.shape
    bf16 = jnp.bfloat16
    quarter = count // 4
    whole = pl.BlockSpec(memory_space=pl.ANY)
    near = pl.BlockSpec(memory_space=pltpu.VMEM)
    band = pltpu.VMEM((count, width), bf16)
    messages = 160
    return pl.pallas_call(
        fused_kernel,
        in_specs=[whole] * 4 + [near] * 2,
        out_specs=near,
        out_shape=pltpu.VMEM((6 * cols + count, width), bf16),
        scratch_shapes=[
            pltpu.VMEM((2, rows // 2, cols), jnp.float32),
            pltpu.VMEM((3, cols, rows), bf16),
            band,
            band,
            pltpu.VMEM((count, cols), bf16),
            band,
            band,
            band,
            band,
            band,
            band,
            pltpu.SemaphoreType.DMA((2,)),
            pltpu.SemaphoreType.DMA((4,)),
            pltpu.SemaphoreType.DMA((messages,)),
            pltpu.SemaphoreType.DMA((messages,)),
        ],
        compiler_params=pltpu.CompilerParams(
            collective_id=0, has_side_effects=True, vmem_limit_bytes=27 * 2**20
        ),
    )(tokens, gate_weight, up_weight, down_weight, in_gain, out_gain)


def emit_kernel(flips, *refs):
    outs, (held, sems) = refs[:3], refs[3:]
    slots, step, cols = held.shape
    width = flips.shape[1]
    steps = width // step

    def out_copy(k, i):
        slot = lax.rem(i, slots)
        top = pl.multiple_of(i * step, step)
        return pltpu.make_async_copy(
            held.at[slot], outs[k % 3].at[k // 3, pl.ds(top, step), :], sems.at[slot]
        )

    for k in range(6):

        def one(i, carry):
            if k == 0:

                @pl.when(i >= slots)
                def _():
                    out_copy(k, i).wait()

            else:
                out_copy(k, i).wait()
            lanes = pl.ds(pl.multiple_of(i * step, step), step)
            held[lax.rem(i, slots)] = flips[k * cols : (k + 1) * cols, lanes].T
            out_copy(k, i).start()
            return carry

        lax.fori_loop(0, steps, one, 0)
    for i in range(slots):
        out_copy(5, steps - slots + i).wait()


def emit(flips, cols):
    width = flips.shape[1]
    near = pl.BlockSpec(memory_space=pltpu.VMEM)
    whole = pl.BlockSpec(memory_space=pl.ANY)
    return pl.pallas_call(
        emit_kernel,
        in_specs=[near],
        out_specs=[whole] * 3,
        out_shape=[jax.ShapeDtypeStruct((2, width, cols), jnp.bfloat16)] * 3,
        scratch_shapes=[
            pltpu.VMEM((8, 256, cols), jnp.bfloat16),
            pltpu.SemaphoreType.DMA((8,)),
        ],
        compiler_params=pltpu.CompilerParams(vmem_limit_bytes=8 * 2**20),
        cost_estimate=pl.CostEstimate(
            flops=10**10, bytes_accessed=12 * cols * width, transcendentals=0
        ),
    )(flips)


def last_kernel(rest, left, right, out_gain, result):
    quarter = result.shape[0]

    def one(i, carry):
        line = pl.ds(pl.multiple_of(i * 32, 32), 32)
        total = rest[line, :].astype(jnp.float32) + left[line, :].astype(jnp.float32)
        total += right[line, :].astype(jnp.float32)
        before = rest[pl.ds(pl.multiple_of(quarter + i * 32, 32), 32), :].astype(jnp.float32)
        after = before + 0.5 * out_gain[1:2, :] * normalize(total)
        result[line, :] = after.astype(jnp.bfloat16)
        return carry

    lax.fori_loop(0, quarter // 32, one, 0)


def last_step(rest, left, right, out_gain):
    near = pl.BlockSpec(memory_space=pltpu.VMEM)
    return pl.pallas_call(
        last_kernel,
        in_specs=[near] * 4,
        out_specs=near,
        out_shape=jax.ShapeDtypeStruct(left.shape, jnp.bfloat16),
        compiler_params=pltpu.CompilerParams(vmem_limit_bytes=8 * 2**20),
    )(rest, left, right, out_gain)


def body(tokens, gate_weight, up_weight, down_weight, in_gain, out_gain):
    groups, halves = lax.axis_size("fs"), lax.axis_size("grp")
    columns = lax.axis_size("tp")
    count, model_width = tokens.shape
    _, rows, cols = gate_weight.shape
    odd = cols % (32 * groups) or rows % 256 or cols % 128 or count % 512 or model_width % 2048
    if odd or halves != 2 or columns != 4 or groups != 4:
        return body_plain(tokens, gate_weight, up_weight, down_weight, in_gain, out_gain)
    flips = fused(tokens, gate_weight, up_weight, down_weight, in_gain, out_gain)
    quarter = count // groups
    base = 6 * cols
    ahead = lax.slice_in_dim(flips, base, base + quarter)
    back = lax.slice_in_dim(flips, base + quarter, base + 2 * quarter)
    rest = lax.slice_in_dim(flips, base + 2 * quarter, base + 4 * quarter)
    left = lax.ppermute(ahead, "fs", [(i, i + 1) for i in range(groups - 1)])
    right = lax.ppermute(back, "fs", [(i + 1, i) for i in range(groups - 1)])
    outs = emit(flips, cols)
    return (*outs, last_step(rest, left, right, out_gain))


def solution(mesh):
    in_specs = (
        P(("grp", "tp"), None),
        P(None, "fs", "tp"),
        P(None, "fs", "tp"),
        P(None, "fs", "tp"),
        P(None, "fs"),
        P(),
    )
    out_specs = (
        P("grp", None, "fs"),
        P("grp", None, "fs"),
        P("grp", None, "fs"),
        P(("grp", "tp", "fs"), None),
    )
    return jax.shard_map(body, mesh=mesh, in_specs=in_specs, out_specs=out_specs, check_vma=False)
```
